32 devices in a mesh: fs: 4 (over z), tp: 4 (over y, x), rep: 2 (over core).
Axes of the slice: x: 2, y: 2, z: 4, core: 2. Of those that a mesh axis runs over, the one named last changes fastest.
Arguments:
- gate_weight: float32 [2048, 5632], P('fs', 'tp'), may hold values from -6 to 6
- gate_momentum: float32 [2048, 5632], P('fs', 'tp'), may hold values from -60 to 60
- gate_grads: float32 [2, 2048, 5632], P('rep', 'fs', 'tp'), may hold values from -3500 to 3500
- gate_rows: float32 [2048], P('fs'), may hold values from 0.3 to 3
- gate_columns: float32 [5632], P('tp'), may hold values from 0.3 to 3
- up_weight: float32 [2048, 5632], P('fs', 'tp'), may hold values from -6 to 6
- up_momentum: float32 [2048, 5632], P('fs', 'tp'), may hold values from -60 to 60
- up_grads: float32 [2, 2048, 5632], P('rep', 'fs', 'tp'), may hold values from -3500 to 3500
- up_rows: float32 [2048], P('fs'), may hold values from 0.3 to 3
- up_columns: float32 [5632], P('tp'), may hold values from 0.3 to 3
- down_weight: float32 [5632, 2048], P('fs', 'tp'), may hold values from -6 to 6
- down_momentum: float32 [5632, 2048], P('fs', 'tp'), may hold values from -60 to 60
- down_grads: float32 [2, 5632, 2048], P('rep', 'fs', 'tp'), may hold values from -3500 to 3500
- down_rows: float32 [5632], P('fs'), may hold values from 0.3 to 3
- down_columns: float32 [2048], P('tp'), may hold values from 0.3 to 3
- mixer_weight: float32 [2048, 2048], P('fs', 'tp'), may hold values from -6 to 6
- mixer_momentum: float32 [2048, 2048], P('fs', 'tp'), may hold values from -60 to 60
- mixer_grads: float32 [2, 2048, 2048], P('rep', 'fs', 'tp'), may hold values from -3500 to 3500
- mixer_rows: float32 [2048], P('fs'), may hold values from 0.3 to 3
- mixer_columns: float32 [2048], P('tp'), may hold values from 0.3 to 3
Outputs:
- gate_weight_next: float32 [2048, 5632], P('fs', 'tp')
- gate_momentum_next: float32 [2048, 5632], P('fs', 'tp')
- gate_rows_next: float32 [2048], P('fs')
- gate_columns_next: float32 [5632], P('tp')
- up_weight_next: float32 [2048, 5632], P('fs', 'tp')
- up_momentum_next: float32 [2048, 5632], P('fs', 'tp')
- up_rows_next: float32 [2048], P('fs')
- up_columns_next: float32 [5632], P('tp')
- down_weight_next: float32 [5632, 2048], P('fs', 'tp')
- down_momentum_next: float32 [5632, 2048], P('fs', 'tp')
- down_rows_next: float32 [5632], P('fs')
- down_columns_next: float32 [2048], P('tp')
- mixer_weight_next: float32 [2048, 2048], P('fs', 'tp')
- mixer_momentum_next: float32 [2048, 2048], P('fs', 'tp')
- mixer_rows_next: float32 [2048], P('fs')
- mixer_columns_next: float32 [2048], P('tp')
The draws below stay inside these ranges and needn't reach their ends.
All inputs are finite; a program needn't handle non-finite values.
Results may differ from the reference program's by a relative error of at most 0.00002.
Values sent between devices are 32-bit elements; how exact they have to be, the bound alone decides.
A program may use at most 128 MiB of HBM per device.

```python
import math
import jax
import jax.numpy as jnp
from jax import lax

D = 2048
FF = 5632
N_REP = 2


def grad_draw(key, salt, height, width):
    base_key = jax.random.fold_in(key, salt)
    keys = jax.random.split(base_key, 5)
    entry_scale = 10.0 ** jax.random.uniform(keys[4], (height, width), jnp.float32, -1.0, 1.0)
    row_scale = 10.0 ** jax.random.uniform(keys[0], (height,), jnp.float32, -0.5, 0.5)
    col_scale = 10.0 ** jax.random.uniform(keys[1], (width,), jnp.float32, -0.5, 0.5)
    values = jnp.clip(jax.random.normal(keys[2], (N_REP, height, width), jnp.float32), -6.0, 6.0)
    row_trend = 3.0 ** (jnp.arange(height, dtype=jnp.float32) / height - 0.5)
    col_trend = 3.0 ** (jnp.arange(width, dtype=jnp.float32) / width - 0.5)
    scales = (row_scale * row_trend)[:, None] * (col_scale * col_trend)[None, :] * entry_scale
    return values * scales[None, :, :]


def momentum_draw(key, salt, height, width):
    base_key = jax.random.fold_in(key, salt)
    keys = jax.random.split(base_key, 2)
    entry_scale = 10.0 ** jax.random.uniform(keys[0], (height, width), jnp.float32, -1.0, 1.0)
    values = jnp.clip(jax.random.normal(keys[1], (height, width), jnp.float32), -6.0, 6.0)
    return values * entry_scale


def draw_gate_grads(key, part):
    return grad_draw(key, 11, D, FF)


def draw_up_grads(key, part):
    return grad_draw(key, 12, D, FF)


def draw_down_grads(key, part):
    return grad_draw(key, 13, FF, D)


def draw_mixer_grads(key, part):
    return grad_draw(key, 14, D, D)


def draw_gate_momentum(key, part):
    return momentum_draw(key, 21, D, FF)


def draw_up_momentum(key, part):
    return momentum_draw(key, 22, D, FF)


def draw_down_momentum(key, part):
    return momentum_draw(key, 23, FF, D)


def draw_mixer_momentum(key, part):
    return momentum_draw(key, 24, D, D)


def level_of(own_key, extent, cuts, least, largest):
    level, own = 1.0, jax.random.fold_in(own_key, 6)
    for axis_at, blocks in cuts:
        steps = jnp.exp(jax.random.uniform(jax.random.fold_in(own, axis_at), (blocks,), jnp.float32, least / len(cuts), largest / len(cuts)))
        level = level * jnp.repeat(steps, extent[axis_at] // blocks).reshape([-1 if axis == axis_at else 1 for axis in range(len(extent))])
    return level


def centred(own_key, extent, scale, most, cuts=(), held_as=jnp.bfloat16):
    loudness = level_of(own_key, extent, cuts, -0.22, 0.18) if cuts else 1.0
    entries = jax.random.normal(own_key, extent, jnp.float32) * scale * loudness
    return jnp.minimum(jnp.maximum(entries, -most), most).astype(held_as)


def setup_inputs(seed: int = 0) -> dict:
    key_of = jax.random.split(jax.random.key(seed), 21)
    gate_weight = centred(key_of[0], (D, FF), 1.0, 6.0, ((0, 4), (1, 4)), jnp.float32)
    gate_momentum = draw_gate_momentum(jax.random.fold_in(key_of[20], 71), 0)
    gate_grads = draw_gate_grads(jax.random.fold_in(key_of[20], 71), 0)
    gate_rows = jnp.clip(jnp.exp(math.log(3.0) - 2.3025851 * jax.random.uniform(key_of[3], (D,), jnp.float32) ** level_of(key_of[3], (D,), ((0, 4),), -0.2, 0.2)), 0.3, 3.0)
    gate_columns = jnp.clip(jnp.exp(math.log(3.0) - 2.3025851 * jax.random.uniform(key_of[4], (FF,), jnp.float32) ** level_of(key_of[4], (FF,), ((0, 4),), -0.2, 0.2)), 0.3, 3.0)
    up_weight = centred(key_of[5], (D, FF), 1.0, 6.0, ((0, 4), (1, 4)), jnp.float32)
    up_momentum = draw_up_momentum(jax.random.fold_in(key_of[20], 71), 0)
    up_grads = draw_up_grads(jax.random.fold_in(key_of[20], 71), 0)
    up_rows = jnp.clip(jnp.exp(math.log(3.0) - 2.3025851 * jax.random.uniform(key_of[8], (D,), jnp.float32) ** level_of(key_of[8], (D,), ((0, 4),), -0.2, 0.2)), 0.3, 3.0)
    up_columns = jnp.clip(jnp.exp(math.log(3.0) - 2.3025851 * jax.random.uniform(key_of[9], (FF,), jnp.float32) ** level_of(key_of[9], (FF,), ((0, 4),), -0.2, 0.2)), 0.3, 3.0)
    down_weight = centred(key_of[10], (FF, D), 1.0, 6.0, ((0, 4), (1, 4)), jnp.float32)
    down_momentum = draw_down_momentum(jax.random.fold_in(key_of[20], 71), 0)
    down_grads = draw_down_grads(jax.random.fold_in(key_of[20], 71), 0)
    down_rows = jnp.clip(jnp.exp(math.log(3.0) - 2.3025851 * jax.random.uniform(key_of[13], (FF,), jnp.float32) ** level_of(key_of[13], (FF,), ((0, 4),), -0.2, 0.2)), 0.3, 3.0)
    down_columns = jnp.clip(jnp.exp(math.log(3.0) - 2.3025851 * jax.random.uniform(key_of[14], (D,), jnp.float32) ** level_of(key_of[14], (D,), ((0, 4),), -0.2, 0.2)), 0.3, 3.0)
    mixer_weight = centred(key_of[15], (D, D), 1.0, 6.0, ((0, 4), (1, 4)), jnp.float32)
    mixer_momentum = draw_mixer_momentum(jax.random.fold_in(key_of[20], 71), 0)
    mixer_grads = draw_mixer_grads(jax.random.fold_in(key_of[20], 71), 0)
    mixer_rows = jnp.clip(jnp.exp(math.log(3.0) - 2.3025851 * jax.random.uniform(key_of[18], (D,), jnp.float32) ** level_of(key_of[18], (D,), ((0, 4),), -0.2, 0.2)), 0.3, 3.0)
    mixer_columns = jnp.clip(jnp.exp(math.log(3.0) - 2.3025851 * jax.random.uniform(key_of[19], (D,), jnp.float32) ** level_of(key_of[19], (D,), ((0, 4),), -0.2, 0.2)), 0.3, 3.0)
    return {"gate_weight": gate_weight, "gate_momentum": gate_momentum, "gate_grads": gate_grads, "gate_rows": gate_rows, "gate_columns": gate_columns, "up_weight": up_weight, "up_momentum": up_momentum, "up_grads": up_grads, "up_rows": up_rows, "up_columns": up_columns, "down_weight": down_weight, "down_momentum": down_momentum, "down_grads": down_grads, "down_rows": down_rows, "down_columns": down_columns, "mixer_weight": mixer_weight, "mixer_momentum": mixer_momentum, "mixer_grads": mixer_grads, "mixer_rows": mixer_rows, "mixer_columns": mixer_columns}


momentum_decay = 0.9
moment_decay = 0.95
clip_level = 0.25
step_rate = 0.1

def update_matrix(weight, momentum, grads, rows, columns):
    grad = lax.optimization_barrier(jnp.sum(grads.astype(jnp.float32), axis=0))
    momentum_next = momentum_decay * momentum + (1.0 - momentum_decay) * grad
    squares = grad * grad
    rows_next = moment_decay * rows + (1.0 - moment_decay) * lax.optimization_barrier(jnp.mean(squares, axis=1))
    columns_next = moment_decay * columns + (1.0 - moment_decay) * lax.optimization_barrier(jnp.mean(squares, axis=0))
    row_mean = jnp.mean(rows_next)
    update = momentum_next * lax.rsqrt(rows_next[:, None] * columns_next[None, :] / row_mean)
    spread = jnp.sqrt(jnp.mean(update * update))
    factor = jnp.maximum(1.0, spread / clip_level)
    weight_next = weight - step_rate * update / factor
    return (weight_next, momentum_next, rows_next, columns_next)

def reference(gate_weight, gate_momentum, gate_grads, gate_rows, gate_columns, up_weight, up_momentum, up_grads, up_rows, up_columns, down_weight, down_momentum, down_grads, down_rows, down_columns, mixer_weight, mixer_momentum, mixer_grads, mixer_rows, mixer_columns):
    first = update_matrix(gate_weight, gate_momentum, gate_grads, gate_rows, gate_columns)
    second = update_matrix(up_weight, up_momentum, up_grads, up_rows, up_columns)
    third = update_matrix(down_weight, down_momentum, down_grads, down_rows, down_columns)
    fourth = update_matrix(mixer_weight, mixer_momentum, mixer_grads, mixer_rows, mixer_columns)
    return (first[0], first[1], first[2], first[3], second[0], second[1], second[2], second[3], third[0], third[1], third[2], third[3], fourth[0], fourth[1], fourth[2], fourth[3])
```

```python
import functools

import jax
import jax.numpy as jnp
from jax import lax
from jax.experimental import pallas as pl
from jax.experimental.pallas import tpu as pltpu
from jax.sharding import PartitionSpec as P

momentum_decay = 0.9
moment_decay = 0.95
clip_level = 0.25
step_rate = 0.1
MESH = pl.DeviceIdType.MESH
LANES = 128


class Plan:
    def __init__(self, height, width):
        rows = LANES if height % LANES == 0 else height
        tiles = width // LANES
        if (height // rows) % 2 and tiles % 2:
            rows //= 2
        self.height, self.width, self.rows, self.tiles = height, width, rows, tiles
        self.chunks = height // rows
        self.by_rows = self.chunks % 2 == 0
        self.own_chunks = self.chunks // 2 if self.by_rows else self.chunks
        self.own_tiles = tiles if self.by_rows else tiles // 2
        self.region = (self.own_chunks * rows, self.own_tiles * LANES)

    def row_at(self, owner, c):
        start = (owner * self.own_chunks + c) * self.rows if self.by_rows else c * self.rows
        return pl.multiple_of(start, self.rows)

    def column_at(self, owner, j=0):
        return j * LANES if self.by_rows else pl.multiple_of((owner * self.own_tiles + j) * LANES, LANES)

    def chunk(self, owner, c):
        return pl.ds(self.row_at(owner, c), self.rows), pl.ds(self.column_at(owner), self.region[1])

    def block(self, owner):
        return pl.ds(self.row_at(owner, 0), self.region[0]), pl.ds(self.column_at(owner), self.region[1])

    def tile(self, owner, c, j):
        return pl.ds(self.row_at(owner, c), self.rows), pl.ds(self.column_at(owner, j), LANES)


def fold(x):
    return jnp.sum(x.reshape(x.shape[0] // 8, 8, x.shape[1]), axis=0)


def to_lanes(x):
    rows = x.shape[0]
    if rows < LANES:
        x = jnp.concatenate([x, jnp.zeros((LANES - rows, LANES), x.dtype)], axis=0)
    return jnp.sum(x.T, axis=0, keepdims=True)


def to_rows(x, rows):
    return jnp.broadcast_to(x, (LANES, LANES)).T[:rows]


def gather_kernel(plans, n_fs, n_tp, *refs):
    n_all = n_fs * n_tp
    ins, refs = refs[:20], refs[20:]
    outs, refs = refs[:20], refs[20:]
    own, refs = refs[:4], refs[4:]
    other, refs = refs[:4], refs[4:]
    row_all, refs = refs[:4], refs[4:]
    column_part, refs = refs[:4], refs[4:]
    column_all, refs = refs[:4], refs[4:]
    row_in, refs = refs[:4], refs[4:]
    column_in, refs = refs[:4], refs[4:]
    (share_all, own_sem, other_send, other_recv, momentum_sem, back_send, back_recv, weight_sem, moment_sem,
     row_send, row_recv, column_send, column_recv, share_send, share_recv, ready, everyone) = refs
    fs, tp, rep = lax.axis_index("fs"), lax.axis_index("tp"), lax.axis_index("rep")
    partner = {"rep": 1 - rep}
    barrier = pltpu.get_barrier_semaphore()

    base = [0]
    for p in plans:
        base.append(base[-1] + p.own_chunks)

    def rows_of(p, c):
        return pl.ds(pl.multiple_of(c * p.rows, p.rows), p.rows)

    def load(k, c):
        p = plans[k]
        r, w = p.chunk(rep, c)
        return pltpu.make_async_copy(ins[5 * k + 2].at[0, r, w], own[k].at[rows_of(p, c)], own_sem.at[base[k] + c])

    def load_momentum(k, c):
        at = plans[k].chunk(rep, c)
        return pltpu.make_async_copy(ins[5 * k + 1].at[at], outs[5 * k + 1].at[at], momentum_sem.at[base[k] + c])

    def send(k, c):
        p = plans[k]
        r, w = p.chunk(1 - rep, c)
        return pltpu.make_async_remote_copy(
            src_ref=ins[5 * k + 2].at[0, r, w], dst_ref=other[k].at[rows_of(p, c)],
            send_sem=other_send.at[base[k] + c], recv_sem=other_recv.at[base[k] + c],
            device_id=partner, device_id_type=MESH)

    def give_back(k, owner):
        at = plans[k].block(owner)
        return pltpu.make_async_remote_copy(
            src_ref=outs[5 * k + 1].at[at], dst_ref=outs[5 * k + 1].at[at],
            send_sem=back_send.at[k], recv_sem=back_recv.at[k],
            device_id=partner, device_id_type=MESH)

    def load_weight(k):
        return pltpu.make_async_copy(ins[5 * k], outs[5 * k], weight_sem.at[k])

    def load_moments(k):
        return (pltpu.make_async_copy(ins[5 * k + 3], row_in[k], moment_sem.at[k]),
                pltpu.make_async_copy(ins[5 * k + 4], column_in[k], moment_sem.at[4 + k]))

    def each(k, f):
        @pl.loop(0, plans[k].own_chunks)
        def _(c):
            f(k, c)

    def place(d):
        lin = lax.rem(fs * n_tp + tp + d, n_all)
        return {"fs": lax.div(lin, n_tp), "tp": lax.rem(lin, n_tp)}

    @pl.when(rep == 1)
    def _():
        pl.semaphore_signal(barrier, inc=1, device_id={"rep": 0}, device_id_type=MESH)

    @pl.when(rep == 0)
    def _():
        pl.semaphore_wait(barrier, 1)
        pl.semaphore_signal(ready, inc=1, device_id={"rep": 1}, device_id_type=MESH)

    @pl.when(rep == 1)
    def _():
        pl.semaphore_wait(ready, 1)

    for k in range(4):
        each(k, lambda k, c: send(k, c).start())

    @pl.when(rep == 1)
    def _():
        @pl.loop(1, n_all)
        def _(d):
            pl.semaphore_signal(barrier, inc=1, device_id=place(d), device_id_type=MESH)

    for k in range(4):
        each(k, lambda k, c: load(k, c).start())
        each(k, lambda k, c: load_momentum(k, c).start())
    for k in range(4):
        for copy in load_moments(k):
            copy.start()
    for k in range(4):
        load_weight(k).start()

    def accumulate(k):
        p = plans[k]
        column_part[k][...] = jnp.zeros_like(column_part[k])

        @pl.loop(0, p.own_chunks)
        def _(c):
            load(k, c).wait()
            load_momentum(k, c).wait()
            send(k, c).wait_recv()
            part = jnp.zeros((p.rows, LANES), jnp.float32)
            for j in range(p.own_tiles):
                at = (rows_of(p, c), pl.ds(j * LANES, LANES))
                full = p.tile(rep, c, j)
                grad = own[k][at] + other[k][at]
                outs[5 * k + 1][full] = momentum_decay * outs[5 * k + 1][full] + (1.0 - momentum_decay) * grad
                square = grad * grad
                part = part + square
                column_part[k][:, pl.ds(j * LANES, LANES)] += fold(square)
            row_all[k][rep, tp, pl.ds(c, 1)] = to_lanes(part)

        for j in range(p.own_tiles):
            column_all[k][rep, fs, pl.ds(j, 1)] = jnp.sum(
                column_part[k][:, pl.ds(j * LANES, LANES)], axis=0, keepdims=True)

    def row_copy(k, d):
        lin = lax.rem(rep * n_tp + tp + d, 2 * n_tp)
        return pltpu.make_async_remote_copy(
            src_ref=row_all[k].at[rep, tp], dst_ref=row_all[k].at[rep, tp],
            send_sem=row_send.at[k, d], recv_sem=row_recv.at[k, d],
            device_id={"rep": lax.div(lin, n_tp), "tp": lax.rem(lin, n_tp)}, device_id_type=MESH)

    def column_copy(k, d):
        lin = lax.rem(rep * n_fs + fs + d, 2 * n_fs)
        return pltpu.make_async_remote_copy(
            src_ref=column_all[k].at[rep, fs], dst_ref=column_all[k].at[rep, fs],
            send_sem=column_send.at[k, d], recv_sem=column_recv.at[k, d],
            device_id={"rep": lax.div(lin, n_fs), "fs": lax.rem(lin, n_fs)}, device_id_type=MESH)

    me = (rep * n_fs + fs) * n_tp + tp

    def share_copy(d):
        lin = lax.rem(me + d, 2 * n_all)
        at = lax.rem(lin, n_all)
        return pltpu.make_async_remote_copy(
            src_ref=share_all.at[me], dst_ref=share_all.at[me],
            send_sem=share_send.at[d], recv_sem=share_recv.at[d],
            device_id={"rep": lax.div(lin, n_all), "fs": lax.div(at, n_tp), "tp": lax.rem(at, n_tp)},
            device_id_type=MESH)

    def moments(k):
        p = plans[k]

        @pl.loop(1, 2 * n_tp)
        def _(d):
            row_copy(k, d).wait_recv()

        @pl.loop(1, 2 * n_fs)
        def _(d):
            column_copy(k, d).wait_recv()

        for copy in load_moments(k):
            copy.wait()
        row_sums = [jnp.sum(row_all[k][q], axis=0) for q in range(2)]
        column_sums = [jnp.sum(column_all[k][q], axis=0) for q in range(2)]
        row_scale = (1.0 - moment_decay) / (p.width * n_tp)
        column_scale = (1.0 - moment_decay) / (p.height * n_fs)
        if p.by_rows:
            for q in range(2):
                at = pl.ds(q * p.own_chunks, p.own_chunks)
                outs[5 * k + 2][at] = moment_decay * row_in[k][at] + row_scale * row_sums[q]
            outs[5 * k + 3][...] = moment_decay * column_in[k][...] + column_scale * (column_sums[0] + column_sums[1])
            mine = outs[5 * k + 2][pl.ds(rep * p.own_chunks, p.own_chunks)]
        else:
            outs[5 * k + 2][...] = moment_decay * row_in[k][...] + row_scale * (row_sums[0] + row_sums[1])
            for q in range(2):
                at = pl.ds(q * p.own_tiles, p.own_tiles)
                outs[5 * k + 3][at] = moment_decay * column_in[k][at] + column_scale * column_sums[q]
            mine = outs[5 * k + 2][...]
        lane = lax.broadcasted_iota(jnp.int32, mine.shape, 1)
        mass = jnp.sum(jnp.where(lane < p.rows, mine, 0.0), axis=0, keepdims=True)
        first_chunk = rep * p.own_chunks if p.by_rows else 0
        first_tile = 0 if p.by_rows else rep * p.own_tiles

        def step(c, sums):
            inverse = to_rows(1.0 / outs[5 * k + 2][pl.ds(first_chunk + c, 1)], p.rows)
            new = []
            for j in range(p.own_tiles):
                m = outs[5 * k + 1][p.tile(rep, c, j)]
                new.append(sums[j] + fold(m * m * inverse))
            return tuple(new)

        zero = jnp.zeros((8, LANES), jnp.float32)
        sums = lax.fori_loop(0, p.own_chunks, step, (zero,) * p.own_tiles)
        share = zero
        for j in range(p.own_tiles):
            share = share + sums[j] / outs[5 * k + 3][pl.ds(first_tile + j, 1)]
        share_all[me, pl.ds(2 * k, 1)] = jnp.sum(share, axis=0, keepdims=True)
        share_all[me, pl.ds(2 * k + 1, 1)] = mass

    for k in range(4):
        accumulate(k)
        if k == 0:
            @pl.when(rep == 1)
            def _():
                pl.semaphore_wait(barrier, n_all - 1)
                pl.semaphore_signal(everyone, inc=1, device_id={"rep": 0}, device_id_type=MESH)

            @pl.when(rep == 0)
            def _():
                pl.semaphore_wait(everyone, 1)

        @pl.loop(1, 2 * n_fs)
        def _(d):
            column_copy(k, d).start()

        @pl.loop(1, 2 * n_tp)
        def _(d):
            row_copy(k, d).start()

    for k in range(4):
        give_back(k, rep).start()
    for k in range(4):
        moments(k)

    @pl.loop(1, 2 * n_all)
    def _(d):
        share_copy(d).start()

    @pl.loop(1, 2 * n_all)
    def _(d):
        share_copy(d).wait_recv()

    total = jnp.sum(jnp.sum(share_all[...], axis=0), axis=1, keepdims=True)
    for k, p in enumerate(plans):
        copies = n_tp if p.by_rows else 2 * n_tp
        row_mean = total[2 * k + 1:2 * k + 2] / (p.height * n_fs * copies)
        spread = jnp.sqrt(row_mean * total[2 * k:2 * k + 1] / (p.height * n_fs * p.width * n_tp))
        factor = jnp.maximum(1.0, spread / clip_level)
        outs[5 * k + 4][...] = jnp.broadcast_to(step_rate * jnp.sqrt(row_mean) / factor, (1, LANES))

    for k in range(4):
        load_weight(k).wait()
        give_back(k, 1 - rep).wait_recv()
        give_back(k, rep).wait_send()
        each(k, lambda k, c: send(k, c).wait_send())

        @pl.loop(1, 2 * n_tp)
        def _(d):
            row_copy(k, d).wait_send()

        @pl.loop(1, 2 * n_fs)
        def _(d):
            column_copy(k, d).wait_send()

    @pl.loop(1, 2 * n_all)
    def _(d):
        share_copy(d).wait_send()


def write_kernel(plans, *refs):
    ins, refs = refs[:20], refs[20:]
    outs, refs = refs[:16], refs[16:]
    weight_next, refs = refs[:4], refs[4:]
    momentum_sem, weight_sem = refs

    def put_momentum(k):
        return pltpu.make_async_copy(ins[5 * k + 1], outs[4 * k + 1], momentum_sem.at[k])

    base = [0]
    for p in plans:
        base.append(base[-1] + p.chunks)

    def span(p, c):
        return pl.ds(pl.multiple_of(c * p.rows, p.rows), p.rows)

    def put_weight(k, c):
        return pltpu.make_async_copy(
            weight_next[k].at[span(plans[k], c)], outs[4 * k].at[span(plans[k], c)], weight_sem.at[base[k] + c])

    for k in range(4):
        put_momentum(k).start()
    for k, p in enumerate(plans):
        outs[4 * k + 2][...] = ins[5 * k + 2][:, :p.rows]
        outs[4 * k + 3][...] = ins[5 * k + 3][...]

        @pl.loop(0, p.chunks)
        def _(c):
            row_factor = to_rows(lax.rsqrt(ins[5 * k + 2][pl.ds(c, 1)]), p.rows)
            for j in range(p.tiles):
                at = (span(p, c), pl.ds(j * LANES, LANES))
                column_factor = lax.rsqrt(ins[5 * k + 3][pl.ds(j, 1)]) * ins[5 * k + 4][...]
                weight_next[k][at] = ins[5 * k][at] - ins[5 * k + 1][at] * row_factor * column_factor
            put_weight(k, c).start()

    for k, p in enumerate(plans):
        put_momentum(k).wait()

        @pl.loop(0, p.chunks)
        def _(c):
            put_weight(k, c).wait()


def body(n_fs, n_tp, *arrays):
    f32 = jnp.float32
    plans = tuple(Plan(*arrays[5 * k].shape) for k in range(4))
    n_all, total, own_total = n_fs * n_tp, sum(p.chunks for p in plans), sum(p.own_chunks for p in plans)
    operands, middle = [], []
    in_specs = []
    hbm, vmem = pl.BlockSpec(memory_space=pl.ANY), pl.BlockSpec(memory_space=pltpu.VMEM)
    for k, p in enumerate(plans):
        w, m, g, r, c = arrays[5 * k:5 * k + 5]
        r = r.reshape(p.chunks, p.rows)
        if p.rows < LANES:
            r = jnp.pad(r, ((0, 0), (0, LANES - p.rows)), constant_values=1.0)
        c = c.reshape(p.tiles, LANES)
        operands += [pltpu.with_memory_space_constraint(x, pltpu.HBM) for x in (w, m, g, r, c)]
        in_specs += [hbm] * 5
        full = (p.height, p.width)
        middle += [pltpu.VMEM(full, f32), pltpu.VMEM(full, f32),
                   pltpu.VMEM((p.chunks, LANES), f32), pltpu.VMEM((p.tiles, LANES), f32), pltpu.VMEM((1, LANES), f32)]
    scratch = [pltpu.VMEM(p.region, f32) for p in plans] * 2
    scratch += [pltpu.VMEM((2, n_tp, p.own_chunks, LANES), f32) for p in plans]
    scratch += [pltpu.VMEM((8, p.region[1]), f32) for p in plans]
    scratch += [pltpu.VMEM((2, n_fs, p.own_tiles, LANES), f32) for p in plans]
    scratch += [pltpu.VMEM((p.chunks, LANES), f32) for p in plans]
    scratch += [pltpu.VMEM((p.tiles, LANES), f32) for p in plans]
    scratch += [pltpu.VMEM((2 * n_all, 8, LANES), f32)]
    dma = pltpu.SemaphoreType.DMA
    scratch += [dma((own_total,)), dma((own_total,)), dma((own_total,)), dma((own_total,))]
    scratch += [dma((4,)), dma((4,)), dma((4,)), dma((8,))]
    scratch += [dma((4, 2 * n_tp)), dma((4, 2 * n_tp)), dma((4, 2 * n_fs)), dma((4, 2 * n_fs))]
    scratch += [dma((2 * n_all,)), dma((2 * n_all,))]
    scratch += [pltpu.SemaphoreType.REGULAR, pltpu.SemaphoreType.REGULAR]
    block = 4 * sum(p.height * p.width for p in plans)
    slack = 8 << 20
    middle = pl.pallas_call(
        functools.partial(gather_kernel, plans, n_fs, n_tp),
        out_shape=middle,
        in_specs=in_specs,
        out_specs=[vmem] * 20,
        scratch_shapes=scratch,
        compiler_params=pltpu.CompilerParams(
            collective_id=0, has_side_effects=True, vmem_limit_bytes=block + slack),
        name="gather",
    )(*operands)
    out_shape, out_specs = [], []
    for p in plans:
        out_shape += [jax.ShapeDtypeStruct((p.height, p.width), f32)] * 2
        out_shape += [jax.ShapeDtypeStruct((p.chunks, p.rows), f32), jax.ShapeDtypeStruct((p.tiles, LANES), f32)]
        out_specs += [hbm, hbm, vmem, vmem]
    outs = pl.pallas_call(
        functools.partial(write_kernel, plans),
        out_shape=out_shape,
        in_specs=[vmem] * 20,
        out_specs=out_specs,
        scratch_shapes=[pltpu.VMEM((p.height, p.width), f32) for p in plans] + [dma((4,)), dma((total,))],
        compiler_params=pltpu.CompilerParams(vmem_limit_bytes=block + slack),
        name="write",
    )(*middle)
    results = []
    for k in range(4):
        results += [outs[4 * k], outs[4 * k + 1], outs[4 * k + 2].reshape(-1), outs[4 * k + 3].reshape(-1)]
    return tuple(results)


def solution(mesh):
    matrix, partial, row, column = P("fs", "tp"), P("rep", "fs", "tp"), P("fs"), P("tp")
    return jax.shard_map(
        functools.partial(body, mesh.shape["fs"], mesh.shape["tp"]),
        mesh=mesh,
        in_specs=(matrix, matrix, partial, row, column) * 4,
        out_specs=(matrix, matrix, row, column) * 4,
        check_vma=False,
    )
```

```python
import functools

import jax
import jax.numpy as jnp
from jax import lax
from jax.experimental import pallas as pl
from jax.experimental.pallas import tpu as pltpu
from jax.sharding import PartitionSpec as P

momentum_decay = 0.9
moment_decay = 0.95
clip_level = 0.25
step_rate = 0.1
MESH = pl.DeviceIdType.MESH
LANES = 128


class Plan:
    def __init__(self, height, width):
        rows = LANES if height % LANES == 0 else height
        tiles = width // LANES
        if (height // rows) % 2 and tiles % 2:
            rows //= 2
        self.height, self.width, self.rows, self.tiles = height, width, rows, tiles
        self.chunks = height // rows
        self.by_rows = self.chunks % 2 == 0
        self.own_chunks = self.chunks // 2 if self.by_rows else self.chunks
        self.own_tiles = tiles if self.by_rows else tiles // 2
        self.region = (self.own_chunks * rows, self.own_tiles * LANES)

    def row_at(self, owner, c):
        start = (owner * self.own_chunks + c) * self.rows if self.by_rows else c * self.rows
        return pl.multiple_of(start, self.rows)

    def column_at(self, owner, j=0):
        return j * LANES if self.by_rows else pl.multiple_of((owner * self.own_tiles + j) * LANES, LANES)

    def chunk(self, owner, c):
        return pl.ds(self.row_at(owner, c), self.rows), pl.ds(self.column_at(owner), self.region[1])

    def block(self, owner):
        return pl.ds(self.row_at(owner, 0), self.region[0]), pl.ds(self.column_at(owner), self.region[1])

    def tile(self, owner, c, j):
        return pl.ds(self.row_at(owner, c), self.rows), pl.ds(self.column_at(owner, j), LANES)


def fold(x):
    return jnp.sum(x.reshape(x.shape[0] // 8, 8, x.shape[1]), axis=0)


def to_lanes(x):
    rows = x.shape[0]
    if rows < LANES:
        x = jnp.concatenate([x, jnp.zeros((LANES - rows, LANES), x.dtype)], axis=0)
    return jnp.sum(x.T, axis=0, keepdims=True)


def to_rows(x, rows):
    return jnp.broadcast_to(x, (LANES, LANES)).T[:rows]


def gather_kernel(plans, n_fs, n_tp, *refs):
    n_all = n_fs * n_tp
    ins, refs = refs[:20], refs[20:]
    outs, refs = refs[:20], refs[20:]
    own, refs = refs[:4], refs[4:]
    other, refs = refs[:4], refs[4:]
    row_all, refs = refs[:4], refs[4:]
    column_part, refs = refs[:4], refs[4:]
    column_all, refs = refs[:4], refs[4:]
    row_in, refs = refs[:4], refs[4:]
    column_in, refs = refs[:4], refs[4:]
    (share_all, own_sem, other_send, other_recv, momentum_sem, back_send, back_recv, weight_sem, moment_sem,
     row_send, row_recv, column_send, column_recv, share_send, share_recv, ready, everyone) = refs
    fs, tp, rep = lax.axis_index("fs"), lax.axis_index("tp"), lax.axis_index("rep")
    partner = {"rep": 1 - rep}
    barrier = pltpu.get_barrier_semaphore()

    def rows_of(p, c):
        return pl.ds(pl.multiple_of(c * p.rows, p.rows), p.rows)

    def load(k):
        r, w = plans[k].block(rep)
        return pltpu.make_async_copy(ins[5 * k + 2].at[0, r, w], own[k], own_sem.at[k])

    def load_momentum(k):
        at = plans[k].block(rep)
        return pltpu.make_async_copy(ins[5 * k + 1].at[at], outs[5 * k + 1].at[at], momentum_sem.at[k])

    def send(k):
        r, w = plans[k].block(1 - rep)
        return pltpu.make_async_remote_copy(
            src_ref=ins[5 * k + 2].at[0, r, w], dst_ref=other[k],
            send_sem=other_send.at[k], recv_sem=other_recv.at[k],
            device_id=partner, device_id_type=MESH)

    def give_back(k, owner):
        at = plans[k].block(owner)
        return pltpu.make_async_remote_copy(
            src_ref=outs[5 * k + 1].at[at], dst_ref=outs[5 * k + 1].at[at],
            send_sem=back_send.at[k], recv_sem=back_recv.at[k],
            device_id=partner, device_id_type=MESH)

    def load_weight(k):
        return pltpu.make_async_copy(ins[5 * k], outs[5 * k], weight_sem.at[k])

    def load_moments(k):
        return (pltpu.make_async_copy(ins[5 * k + 3], row_in[k], moment_sem.at[k]),
                pltpu.make_async_copy(ins[5 * k + 4], column_in[k], moment_sem.at[4 + k]))

    def wait_for(slots, n, sem):
        some = slots.at[pl.ds(0, n)]
        pltpu.make_async_copy(some, some, sem).wait()

    def place(d):
        lin = lax.rem(fs * n_tp + tp + d, n_all)
        return {"fs": lax.div(lin, n_tp), "tp": lax.rem(lin, n_tp)}

    @pl.when(rep == 1)
    def _():
        pl.semaphore_signal(barrier, inc=1, device_id={"rep": 0}, device_id_type=MESH)

    @pl.when(rep == 0)
    def _():
        pl.semaphore_wait(barrier, 1)
        pl.semaphore_signal(ready, inc=1, device_id={"rep": 1}, device_id_type=MESH)

    @pl.when(rep == 1)
    def _():
        pl.semaphore_wait(ready, 1)

    for k in range(4):
        send(k).start()

    @pl.when(rep == 1)
    def _():
        @pl.loop(1, n_all)
        def _(d):
            pl.semaphore_signal(barrier, inc=1, device_id=place(d), device_id_type=MESH)

    for k in range(4):
        load(k).start()
        load_momentum(k).start()
    for k in range(4):
        for copy in load_moments(k):
            copy.start()

    def accumulate(k):
        p = plans[k]
        column_part[k][...] = jnp.zeros_like(column_part[k])
        load(k).wait()
        load_momentum(k).wait()
        send(k).wait_recv()

        @pl.loop(0, p.own_chunks)
        def _(c):
            part = jnp.zeros((p.rows, LANES), jnp.float32)
            for j in range(p.own_tiles):
                at = (rows_of(p, c), pl.ds(j * LANES, LANES))
                full = p.tile(rep, c, j)
                grad = own[k][at] + other[k][at]
                outs[5 * k + 1][full] = momentum_decay * outs[5 * k + 1][full] + (1.0 - momentum_decay) * grad
                square = grad * grad
                part = part + square
                column_part[k][:, pl.ds(j * LANES, LANES)] += fold(square)
            row_all[k][rep * n_tp + tp, pl.ds(c, 1)] = to_lanes(part)

        for j in range(p.own_tiles):
            column_all[k][rep * n_fs + fs, pl.ds(j, 1)] = jnp.sum(
                column_part[k][:, pl.ds(j * LANES, LANES)], axis=0, keepdims=True)

    def row_copy(k, d):
        lin = lax.rem(rep * n_tp + tp + d, 2 * n_tp)
        return pltpu.make_async_remote_copy(
            src_ref=row_all[k].at[rep * n_tp + tp], dst_ref=row_all[k].at[rep * n_tp + tp],
            send_sem=row_send.at[k], recv_sem=row_recv.at[k],
            device_id={"rep": lax.div(lin, n_tp), "tp": lax.rem(lin, n_tp)}, device_id_type=MESH)

    def column_copy(k, d):
        lin = lax.rem(rep * n_fs + fs + d, 2 * n_fs)
        return pltpu.make_async_remote_copy(
            src_ref=column_all[k].at[rep * n_fs + fs], dst_ref=column_all[k].at[rep * n_fs + fs],
            send_sem=column_send.at[k], recv_sem=column_recv.at[k],
            device_id={"rep": lax.div(lin, n_fs), "fs": lax.rem(lin, n_fs)}, device_id_type=MESH)

    me = (rep * n_fs + fs) * n_tp + tp

    def share_copy(d):
        lin = lax.rem(me + d, 2 * n_all)
        at = lax.rem(lin, n_all)
        return pltpu.make_async_remote_copy(
            src_ref=share_all.at[me], dst_ref=share_all.at[me],
            send_sem=share_send, recv_sem=share_recv,
            device_id={"rep": lax.div(lin, n_all), "fs": lax.div(at, n_tp), "tp": lax.rem(at, n_tp)},
            device_id_type=MESH)

    def moments(k):
        p = plans[k]

        wait_for(row_all[k], 2 * n_tp - 1, row_recv.at[k])
        wait_for(column_all[k], 2 * n_fs - 1, column_recv.at[k])
        for copy in load_moments(k):
            copy.wait()
        row_sums = [jnp.sum(row_all[k][pl.ds(q * n_tp, n_tp)], axis=0) for q in range(2)]
        column_sums = [jnp.sum(column_all[k][pl.ds(q * n_fs, n_fs)], axis=0) for q in range(2)]
        row_scale = (1.0 - moment_decay) / (p.width * n_tp)
        column_scale = (1.0 - moment_decay) / (p.height * n_fs)
        if p.by_rows:
            for q in range(2):
                at = pl.ds(q * p.own_chunks, p.own_chunks)
                outs[5 * k + 2][at] = moment_decay * row_in[k][at] + row_scale * row_sums[q]
            outs[5 * k + 3][...] = moment_decay * column_in[k][...] + column_scale * (column_sums[0] + column_sums[1])
            mine = outs[5 * k + 2][pl.ds(rep * p.own_chunks, p.own_chunks)]
        else:
            outs[5 * k + 2][...] = moment_decay * row_in[k][...] + row_scale * (row_sums[0] + row_sums[1])
            for q in range(2):
                at = pl.ds(q * p.own_tiles, p.own_tiles)
                outs[5 * k + 3][at] = moment_decay * column_in[k][at] + column_scale * column_sums[q]
            mine = outs[5 * k + 2][...]
        lane = lax.broadcasted_iota(jnp.int32, mine.shape, 1)
        mass = jnp.sum(jnp.where(lane < p.rows, mine, 0.0), axis=0, keepdims=True)
        first_chunk = rep * p.own_chunks if p.by_rows else 0
        first_tile = 0 if p.by_rows else rep * p.own_tiles

        def step(c, sums):
            inverse = to_rows(1.0 / outs[5 * k + 2][pl.ds(first_chunk + c, 1)], p.rows)
            new = []
            for j in range(p.own_tiles):
                m = outs[5 * k + 1][p.tile(rep, c, j)]
                new.append(sums[j] + fold(m * m * inverse))
            return tuple(new)

        zero = jnp.zeros((8, LANES), jnp.float32)
        sums = lax.fori_loop(0, p.own_chunks, step, (zero,) * p.own_tiles)
        share = zero
        for j in range(p.own_tiles):
            share = share + sums[j] / outs[5 * k + 3][pl.ds(first_tile + j, 1)]
        share_all[me, pl.ds(2 * k, 1)] = jnp.sum(share, axis=0, keepdims=True)
        share_all[me, pl.ds(2 * k + 1, 1)] = mass

    for k in range(4):
        accumulate(k)
        if k == 0:
            @pl.when(rep == 1)
            def _():
                pl.semaphore_wait(barrier, n_all - 1)
                pl.semaphore_signal(everyone, inc=1, device_id={"rep": 0}, device_id_type=MESH)

            @pl.when(rep == 0)
            def _():
                pl.semaphore_wait(everyone, 1)

        @pl.loop(1, 2 * n_fs)
        def _(d):
            column_copy(k, d).start()

        @pl.loop(1, 2 * n_tp)
        def _(d):
            row_copy(k, d).start()

    for k in range(4):
        give_back(k, rep).start()
    for k in range(4):
        load_weight(k).start()
    for k in range(4):
        moments(k)

    @pl.loop(1, 2 * n_all)
    def _(d):
        share_copy(d).start()

    wait_for(share_all, 2 * n_all - 1, share_recv)

    total = jnp.sum(jnp.sum(share_all[...], axis=0), axis=1, keepdims=True)
    for k, p in enumerate(plans):
        copies = n_tp if p.by_rows else 2 * n_tp
        row_mean = total[2 * k + 1:2 * k + 2] / (p.height * n_fs * copies)
        spread = jnp.sqrt(row_mean * total[2 * k:2 * k + 1] / (p.height * n_fs * p.width * n_tp))
        factor = jnp.maximum(1.0, spread / clip_level)
        outs[5 * k + 4][...] = jnp.broadcast_to(step_rate * jnp.sqrt(row_mean) / factor, (1, LANES))

    for k in range(4):
        load_weight(k).wait()
        give_back(k, 1 - rep).wait_recv()
        give_back(k, rep).wait_send()
        send(k).wait_send()
        wait_for(row_all[k], 2 * n_tp - 1, row_send.at[k])
        wait_for(column_all[k], 2 * n_fs - 1, column_send.at[k])
    wait_for(share_all, 2 * n_all - 1, share_send)


def write_kernel(plans, *refs):
    ins, refs = refs[:20], refs[20:]
    outs, refs = refs[:16], refs[16:]
    weight_next, refs = refs[:4], refs[4:]
    momentum_sem, weight_sem = refs

    def put_momentum(k):
        return pltpu.make_async_copy(ins[5 * k + 1], outs[4 * k + 1], momentum_sem.at[k])

    def span(p, c):
        return pl.ds(pl.multiple_of(c * p.rows, p.rows), p.rows)

    def put_weight(k, c):
        return pltpu.make_async_copy(
            weight_next[k].at[span(plans[k], c)], outs[4 * k].at[span(plans[k], c)], weight_sem.at[k])

    for k in range(4):
        put_momentum(k).start()
    for k, p in enumerate(plans):
        outs[4 * k + 2][...] = ins[5 * k + 2][:, :p.rows]
        outs[4 * k + 3][...] = ins[5 * k + 3][...]

        @pl.loop(0, p.chunks)
        def _(c):
            row_factor = to_rows(lax.rsqrt(ins[5 * k + 2][pl.ds(c, 1)]), p.rows)
            for j in range(p.tiles):
                at = (span(p, c), pl.ds(j * LANES, LANES))
                column_factor = lax.rsqrt(ins[5 * k + 3][pl.ds(j, 1)]) * ins[5 * k + 4][...]
                weight_next[k][at] = ins[5 * k][at] - ins[5 * k + 1][at] * row_factor * column_factor
            put_weight(k, c).start()

    for k in range(4):
        put_momentum(k).wait()
        pltpu.make_async_copy(weight_next[k], outs[4 * k], weight_sem.at[k]).wait()


def body(n_fs, n_tp, *arrays):
    f32 = jnp.float32
    plans = tuple(Plan(*arrays[5 * k].shape) for k in range(4))
    n_all = n_fs * n_tp
    operands, middle = [], []
    in_specs = []
    hbm, vmem = pl.BlockSpec(memory_space=pl.ANY), pl.BlockSpec(memory_space=pltpu.VMEM)
    for k, p in enumerate(plans):
        w, m, g, r, c = arrays[5 * k:5 * k + 5]
        r = r.reshape(p.chunks, p.rows)
        if p.rows < LANES:
            r = jnp.pad(r, ((0, 0), (0, LANES - p.rows)), constant_values=1.0)
        c = c.reshape(p.tiles, LANES)
        operands += [pltpu.with_memory_space_constraint(x, pltpu.HBM) for x in (w, m, g, r, c)]
        in_specs += [hbm] * 5
        full = (p.height, p.width)
        middle += [pltpu.VMEM(full, f32), pltpu.VMEM(full, f32),
                   pltpu.VMEM((p.chunks, LANES), f32), pltpu.VMEM((p.tiles, LANES), f32), pltpu.VMEM((1, LANES), f32)]
    scratch = [pltpu.VMEM(p.region, f32) for p in plans] * 2
    scratch += [pltpu.VMEM((2 * n_tp, p.own_chunks, LANES), f32) for p in plans]
    scratch += [pltpu.VMEM((8, p.region[1]), f32) for p in plans]
    scratch += [pltpu.VMEM((2 * n_fs, p.own_tiles, LANES), f32) for p in plans]
    scratch += [pltpu.VMEM((p.chunks, LANES), f32) for p in plans]
    scratch += [pltpu.VMEM((p.tiles, LANES), f32) for p in plans]
    scratch += [pltpu.VMEM((2 * n_all, 8, LANES), f32)]
    dma = pltpu.SemaphoreType.DMA
    scratch += [dma((4,))] * 7 + [dma((8,))] + [dma((4,))] * 4 + [dma, dma]
    scratch += [pltpu.SemaphoreType.REGULAR, pltpu.SemaphoreType.REGULAR]
    block = 4 * sum(p.height * p.width for p in plans)
    slack = 8 << 20
    middle = pl.pallas_call(
        functools.partial(gather_kernel, plans, n_fs, n_tp),
        out_shape=middle,
        in_specs=in_specs,
        out_specs=[vmem] * 20,
        scratch_shapes=scratch,
        compiler_params=pltpu.CompilerParams(
            collective_id=0, has_side_effects=True, vmem_limit_bytes=block + slack),
        name="gather",
    )(*operands)
    out_shape, out_specs = [], []
    for p in plans:
        out_shape += [jax.ShapeDtypeStruct((p.height, p.width), f32)] * 2
        out_shape += [jax.ShapeDtypeStruct((p.chunks, p.rows), f32), jax.ShapeDtypeStruct((p.tiles, LANES), f32)]
        out_specs += [hbm, hbm, vmem, vmem]
    outs = pl.pallas_call(
        functools.partial(write_kernel, plans),
        out_shape=out_shape,
        in_specs=[vmem] * 20,
        out_specs=out_specs,
        scratch_shapes=[pltpu.VMEM((p.height, p.width), f32) for p in plans] + [dma((4,)), dma((4,))],
        compiler_params=pltpu.CompilerParams(vmem_limit_bytes=block + slack),
        name="write",
    )(*middle)
    results = []
    for k in range(4):
        results += [outs[4 * k], outs[4 * k + 1], outs[4 * k + 2].reshape(-1), outs[4 * k + 3].reshape(-1)]
    return tuple(results)


def solution(mesh):
    matrix, partial, row, column = P("fs", "tp"), P("rep", "fs", "tp"), P("fs"), P("tp")
    return jax.shard_map(
        functools.partial(body, mesh.shape["fs"], mesh.shape["tp"]),
        mesh=mesh,
        in_specs=(matrix, matrix, partial, row, column) * 4,
        out_specs=(matrix, matrix, row, column) * 4,
        check_vma=False,
    )
```

```python
import functools

import jax
import jax.numpy as jnp
from jax import lax
from jax.experimental import pallas as pl
from jax.experimental.pallas import tpu as pltpu
from jax.sharding import PartitionSpec as P

momentum_decay = 0.9
moment_decay = 0.95
clip_level = 0.25
step_rate = 0.1
MESH = pl.DeviceIdType.MESH
LANES = 128


class Plan:
    def __init__(self, height, width):
        rows = LANES if height % LANES == 0 else height
        tiles = width // LANES
        if (height // rows) % 2 and tiles % 2:
            rows //= 2
        self.height, self.width, self.rows, self.tiles = height, width, rows, tiles
        self.chunks = height // rows
        self.by_rows = self.chunks % 2 == 0
        self.own_chunks = self.chunks // 2 if self.by_rows else self.chunks
        self.own_tiles = tiles if self.by_rows else tiles // 2
        self.region = (self.own_chunks * rows, self.own_tiles * LANES)
        cut = (self.own_chunks + 1) // 2
        self.pieces = [(0, cut)] + ([(cut, self.own_chunks)] if cut < self.own_chunks else [])

    def row_at(self, owner, c):
        start = (owner * self.own_chunks + c) * self.rows if self.by_rows else c * self.rows
        return pl.multiple_of(start, self.rows)

    def column_at(self, owner, j=0):
        return j * LANES if self.by_rows else pl.multiple_of((owner * self.own_tiles + j) * LANES, LANES)

    def part(self, owner, first, last):
        return pl.ds(self.row_at(owner, first), (last - first) * self.rows), pl.ds(self.column_at(owner), self.region[1])

    def block(self, owner):
        return pl.ds(self.row_at(owner, 0), self.region[0]), pl.ds(self.column_at(owner), self.region[1])

    def tile(self, owner, c, j):
        return pl.ds(self.row_at(owner, c), self.rows), pl.ds(self.column_at(owner, j), LANES)


def fold(x):
    return jnp.sum(x.reshape(x.shape[0] // 8, 8, x.shape[1]), axis=0)


def to_lanes(x):
    rows = x.shape[0]
    if rows < LANES:
        x = jnp.concatenate([x, jnp.zeros((LANES - rows, LANES), x.dtype)], axis=0)
    return jnp.sum(x.T, axis=0, keepdims=True)


def to_rows(x, rows):
    return jnp.broadcast_to(x, (LANES, LANES)).T[:rows]


def gather_kernel(plans, n_fs, n_tp, *refs):
    n_all = n_fs * n_tp
    ins, refs = refs[:20], refs[20:]
    outs, refs = refs[:20], refs[20:]
    own, refs = refs[:4], refs[4:]
    other, refs = refs[:4], refs[4:]
    row_all, refs = refs[:4], refs[4:]
    column_part, refs = refs[:4], refs[4:]
    column_all, refs = refs[:4], refs[4:]
    row_in, refs = refs[:4], refs[4:]
    column_in, refs = refs[:4], refs[4:]
    (share_all, own_sem, other_send, other_recv, momentum_sem, back_send, back_recv, weight_sem, moment_sem,
     row_send, row_recv, column_send, column_recv, share_send, share_recv, ready, everyone) = refs
    fs, tp, rep = lax.axis_index("fs"), lax.axis_index("tp"), lax.axis_index("rep")
    partner = {"rep": 1 - rep}
    barrier = pltpu.get_barrier_semaphore()

    def rows_of(p, c):
        return pl.ds(pl.multiple_of(c * p.rows, p.rows), p.rows)

    def load(k):
        r, w = plans[k].block(rep)
        return pltpu.make_async_copy(ins[5 * k + 2].at[0, r, w], own[k], own_sem.at[k])

    def load_momentum(k):
        at = plans[k].block(rep)
        return pltpu.make_async_copy(ins[5 * k + 1].at[at], outs[5 * k + 1].at[at], momentum_sem.at[k])

    def send(k, i):
        p = plans[k]
        first, last = p.pieces[i]
        r, w = p.part(1 - rep, first, last)
        return pltpu.make_async_remote_copy(
            src_ref=ins[5 * k + 2].at[0, r, w], dst_ref=other[k].at[pl.ds(first * p.rows, (last - first) * p.rows)],
            send_sem=other_send.at[k], recv_sem=other_recv.at[k, i],
            device_id=partner, device_id_type=MESH)

    def give_back(k, owner):
        at = plans[k].block(owner)
        return pltpu.make_async_remote_copy(
            src_ref=outs[5 * k + 1].at[at], dst_ref=outs[5 * k + 1].at[at],
            send_sem=back_send.at[k], recv_sem=back_recv.at[k],
            device_id=partner, device_id_type=MESH)

    def load_weight(k):
        return pltpu.make_async_copy(ins[5 * k], outs[5 * k], weight_sem.at[k])

    def load_moments(k):
        return (pltpu.make_async_copy(ins[5 * k + 3], row_in[k], moment_sem.at[k]),
                pltpu.make_async_copy(ins[5 * k + 4], column_in[k], moment_sem.at[4 + k]))

    def wait_for(slots, n, sem):
        some = slots.at[pl.ds(0, n)]
        pltpu.make_async_copy(some, some, sem).wait()

    def place(d):
        lin = lax.rem(fs * n_tp + tp + d, n_all)
        return {"fs": lax.div(lin, n_tp), "tp": lax.rem(lin, n_tp)}

    @pl.when(rep == 1)
    def _():
        pl.semaphore_signal(barrier, inc=1, device_id={"rep": 0}, device_id_type=MESH)

    @pl.when(rep == 0)
    def _():
        pl.semaphore_wait(barrier, 1)
        pl.semaphore_signal(ready, inc=1, device_id={"rep": 1}, device_id_type=MESH)

    @pl.when(rep == 1)
    def _():
        pl.semaphore_wait(ready, 1)

    for k, p in enumerate(plans):
        for i in range(len(p.pieces)):
            send(k, i).start()

    @pl.when(rep == 1)
    def _():
        @pl.loop(1, n_all)
        def _(d):
            pl.semaphore_signal(barrier, inc=1, device_id=place(d), device_id_type=MESH)

    for k in range(4):
        load(k).start()
        load_momentum(k).start()
    for k in range(4):
        for copy in load_moments(k):
            copy.start()

    def accumulate(k):
        p = plans[k]
        column_part[k][...] = jnp.zeros_like(column_part[k])
        load(k).wait()
        load_momentum(k).wait()

        def step(c):
            part = jnp.zeros((p.rows, LANES), jnp.float32)
            for j in range(p.own_tiles):
                at = (rows_of(p, c), pl.ds(j * LANES, LANES))
                full = p.tile(rep, c, j)
                grad = own[k][at] + other[k][at]
                outs[5 * k + 1][full] = momentum_decay * outs[5 * k + 1][full] + (1.0 - momentum_decay) * grad
                square = grad * grad
                part = part + square
                column_part[k][:, pl.ds(j * LANES, LANES)] += fold(square)
            row_all[k][rep * n_tp + tp, pl.ds(c, 1)] = to_lanes(part)

        for i, (first, last) in enumerate(p.pieces):
            send(k, i).wait_recv()
            pl.loop(first, last)(step)

        for j in range(p.own_tiles):
            column_all[k][rep * n_fs + fs, pl.ds(j, 1)] = jnp.sum(
                column_part[k][:, pl.ds(j * LANES, LANES)], axis=0, keepdims=True)

    def row_copy(k, d):
        lin = lax.rem(rep * n_tp + tp + d, 2 * n_tp)
        return pltpu.make_async_remote_copy(
            src_ref=row_all[k].at[rep * n_tp + tp], dst_ref=row_all[k].at[rep * n_tp + tp],
            send_sem=row_send.at[k], recv_sem=row_recv.at[k],
            device_id={"rep": lax.div(lin, n_tp), "tp": lax.rem(lin, n_tp)}, device_id_type=MESH)

    def column_copy(k, d):
        lin = lax.rem(rep * n_fs + fs + d, 2 * n_fs)
        return pltpu.make_async_remote_copy(
            src_ref=column_all[k].at[rep * n_fs + fs], dst_ref=column_all[k].at[rep * n_fs + fs],
            send_sem=column_send.at[k], recv_sem=column_recv.at[k],
            device_id={"rep": lax.div(lin, n_fs), "fs": lax.rem(lin, n_fs)}, device_id_type=MESH)

    me = (fs * n_tp + tp) * 2 + rep

    def share_copy(d):
        lin = lax.rem(me + d, 2 * n_all)
        at = lax.div(lin, 2)
        return pltpu.make_async_remote_copy(
            src_ref=share_all.at[me], dst_ref=share_all.at[me],
            send_sem=share_send, recv_sem=share_recv,
            device_id={"rep": lax.rem(lin, 2), "fs": lax.div(at, n_tp), "tp": lax.rem(at, n_tp)},
            device_id_type=MESH)

    def moments(k):
        p = plans[k]

        wait_for(row_all[k], 2 * n_tp - 1, row_recv.at[k])
        wait_for(column_all[k], 2 * n_fs - 1, column_recv.at[k])
        for copy in load_moments(k):
            copy.wait()
        row_sums = [jnp.sum(row_all[k][pl.ds(q * n_tp, n_tp)], axis=0) for q in range(2)]
        column_sums = [jnp.sum(column_all[k][pl.ds(q * n_fs, n_fs)], axis=0) for q in range(2)]
        row_scale = (1.0 - moment_decay) / (p.width * n_tp)
        column_scale = (1.0 - moment_decay) / (p.height * n_fs)
        if p.by_rows:
            for q in range(2):
                at = pl.ds(q * p.own_chunks, p.own_chunks)
                outs[5 * k + 2][at] = moment_decay * row_in[k][at] + row_scale * row_sums[q]
            outs[5 * k + 3][...] = moment_decay * column_in[k][...] + column_scale * (column_sums[0] + column_sums[1])
            mine = outs[5 * k + 2][pl.ds(rep * p.own_chunks, p.own_chunks)]
        else:
            outs[5 * k + 2][...] = moment_decay * row_in[k][...] + row_scale * (row_sums[0] + row_sums[1])
            for q in range(2):
                at = pl.ds(q * p.own_tiles, p.own_tiles)
                outs[5 * k + 3][at] = moment_decay * column_in[k][at] + column_scale * column_sums[q]
            mine = outs[5 * k + 2][...]
        lane = lax.broadcasted_iota(jnp.int32, mine.shape, 1)
        mass = jnp.sum(jnp.where(lane < p.rows, mine, 0.0), axis=0, keepdims=True)
        first_chunk = rep * p.own_chunks if p.by_rows else 0
        first_tile = 0 if p.by_rows else rep * p.own_tiles

        def step(c, sums):
            inverse = to_rows(1.0 / outs[5 * k + 2][pl.ds(first_chunk + c, 1)], p.rows)
            new = []
            for j in range(p.own_tiles):
                m = outs[5 * k + 1][p.tile(rep, c, j)]
                new.append(sums[j] + fold(m * m * inverse))
            return tuple(new)

        zero = jnp.zeros((8, LANES), jnp.float32)
        sums = lax.fori_loop(0, p.own_chunks, step, (zero,) * p.own_tiles)
        share = zero
        for j in range(p.own_tiles):
            share = share + sums[j] / outs[5 * k + 3][pl.ds(first_tile + j, 1)]
        share_all[me, pl.ds(2 * k, 1)] = jnp.sum(share, axis=0, keepdims=True)
        share_all[me, pl.ds(2 * k + 1, 1)] = mass

    for k in range(4):
        accumulate(k)
        if k == 0:
            @pl.when(rep == 1)
            def _():
                pl.semaphore_wait(barrier, n_all - 1)
                pl.semaphore_signal(everyone, inc=1, device_id={"rep": 0}, device_id_type=MESH)

            @pl.when(rep == 0)
            def _():
                pl.semaphore_wait(everyone, 1)

        @pl.loop(1, 2 * n_fs)
        def _(d):
            column_copy(k, d).start()

        @pl.loop(1, 2 * n_tp)
        def _(d):
            row_copy(k, d).start()

    for k in range(4):
        give_back(k, rep).start()
    for k in range(4):
        load_weight(k).start()
    for k in range(4):
        moments(k)

    @pl.loop(1, 2 * n_all)
    def _(d):
        share_copy(d).start()

    wait_for(share_all, 2 * n_all - 1, share_recv)

    total = jnp.sum(jnp.sum(share_all[...], axis=0), axis=1, keepdims=True)
    for k, p in enumerate(plans):
        copies = n_tp if p.by_rows else 2 * n_tp
        row_mean = total[2 * k + 1:2 * k + 2] / (p.height * n_fs * copies)
        spread = jnp.sqrt(row_mean * total[2 * k:2 * k + 1] / (p.height * n_fs * p.width * n_tp))
        factor = jnp.maximum(1.0, spread / clip_level)
        outs[5 * k + 4][...] = jnp.broadcast_to(step_rate * jnp.sqrt(row_mean) / factor, (1, LANES))

    for k in range(4):
        load_weight(k).wait()
        give_back(k, 1 - rep).wait_recv()
        give_back(k, rep).wait_send()
        pltpu.make_async_copy(other[k], other[k], other_send.at[k]).wait()
        wait_for(row_all[k], 2 * n_tp - 1, row_send.at[k])
        wait_for(column_all[k], 2 * n_fs - 1, column_send.at[k])
    wait_for(share_all, 2 * n_all - 1, share_send)


def write_kernel(plans, *refs):
    ins, refs = refs[:20], refs[20:]
    outs, refs = refs[:16], refs[16:]
    weight_next, refs = refs[:4], refs[4:]
    momentum_sem, weight_sem = refs

    def put_momentum(k):
        return pltpu.make_async_copy(ins[5 * k + 1], outs[4 * k + 1], momentum_sem.at[k])

    def span(p, c):
        return pl.ds(pl.multiple_of(c * p.rows, p.rows), p.rows)

    def put_weight(k, c):
        return pltpu.make_async_copy(
            weight_next[k].at[span(plans[k], c)], outs[4 * k].at[span(plans[k], c)], weight_sem.at[k])

    for k in range(4):
        put_momentum(k).start()
    for k, p in enumerate(plans):
        outs[4 * k + 2][...] = ins[5 * k + 2][:, :p.rows]
        outs[4 * k + 3][...] = ins[5 * k + 3][...]

        @pl.loop(0, p.chunks)
        def _(c):
            row_factor = to_rows(lax.rsqrt(ins[5 * k + 2][pl.ds(c, 1)]), p.rows)
            for j in range(p.tiles):
                at = (span(p, c), pl.ds(j * LANES, LANES))
                column_factor = lax.rsqrt(ins[5 * k + 3][pl.ds(j, 1)]) * ins[5 * k + 4][...]
                weight_next[k][at] = ins[5 * k][at] - ins[5 * k + 1][at] * row_factor * column_factor
            put_weight(k, c).start()

    for k in range(4):
        put_momentum(k).wait()
        pltpu.make_async_copy(weight_next[k], outs[4 * k], weight_sem.at[k]).wait()


def body(n_fs, n_tp, *arrays):
    f32 = jnp.float32
    plans = tuple(Plan(*arrays[5 * k].shape) for k in range(4))
    n_all = n_fs * n_tp
    operands, middle = [], []
    in_specs = []
    hbm, vmem = pl.BlockSpec(memory_space=pl.ANY), pl.BlockSpec(memory_space=pltpu.VMEM)
    for k, p in enumerate(plans):
        w, m, g, r, c = arrays[5 * k:5 * k + 5]
        r = r.reshape(p.chunks, p.rows)
        if p.rows < LANES:
            r = jnp.pad(r, ((0, 0), (0, LANES - p.rows)), constant_values=1.0)
        c = c.reshape(p.tiles, LANES)
        operands += [pltpu.with_memory_space_constraint(x, pltpu.HBM) for x in (w, m, g, r, c)]
        in_specs += [hbm] * 5
        full = (p.height, p.width)
        middle += [pltpu.VMEM(full, f32), pltpu.VMEM(full, f32),
                   pltpu.VMEM((p.chunks, LANES), f32), pltpu.VMEM((p.tiles, LANES), f32), pltpu.VMEM((1, LANES), f32)]
    scratch = [pltpu.VMEM(p.region, f32) for p in plans] * 2
    scratch += [pltpu.VMEM((2 * n_tp, p.own_chunks, LANES), f32) for p in plans]
    scratch += [pltpu.VMEM((8, p.region[1]), f32) for p in plans]
    scratch += [pltpu.VMEM((2 * n_fs, p.own_tiles, LANES), f32) for p in plans]
    scratch += [pltpu.VMEM((p.chunks, LANES), f32) for p in plans]
    scratch += [pltpu.VMEM((p.tiles, LANES), f32) for p in plans]
    scratch += [pltpu.VMEM((2 * n_all, 8, LANES), f32)]
    dma = pltpu.SemaphoreType.DMA
    scratch += [dma((4,))] * 2 + [dma((4, 2))] + [dma((4,))] * 4 + [dma((8,))] + [dma((4,))] * 4 + [dma, dma]
    scratch += [pltpu.SemaphoreType.REGULAR, pltpu.SemaphoreType.REGULAR]
    block = 4 * sum(p.height * p.width for p in plans)
    slack = 8 << 20
    middle = pl.pallas_call(
        functools.partial(gather_kernel, plans, n_fs, n_tp),
        out_shape=middle,
        in_specs=in_specs,
        out_specs=[vmem] * 20,
        scratch_shapes=scratch,
        compiler_params=pltpu.CompilerParams(
            collective_id=0, has_side_effects=True, vmem_limit_bytes=block + slack),
        name="gather",
    )(*operands)
    out_shape, out_specs = [], []
    for p in plans:
        out_shape += [jax.ShapeDtypeStruct((p.height, p.width), f32)] * 2
        out_shape += [jax.ShapeDtypeStruct((p.chunks, p.rows), f32), jax.ShapeDtypeStruct((p.tiles, LANES), f32)]
        out_specs += [hbm, hbm, vmem, vmem]
    outs = pl.pallas_call(
        functools.partial(write_kernel, plans),
        out_shape=out_shape,
        in_specs=[vmem] * 20,
        out_specs=out_specs,
        scratch_shapes=[pltpu.VMEM((p.height, p.width), f32) for p in plans] + [dma((4,)), dma((4,))],
        compiler_params=pltpu.CompilerParams(vmem_limit_bytes=block + slack),
        name="write",
    )(*middle)
    results = []
    for k in range(4):
        results += [outs[4 * k], outs[4 * k + 1], outs[4 * k + 2].reshape(-1), outs[4 * k + 3].reshape(-1)]
    return tuple(results)


def solution(mesh):
    matrix, partial, row, column = P("fs", "tp"), P("rep", "fs", "tp"), P("fs"), P("tp")
    return jax.shard_map(
        functools.partial(body, mesh.shape["fs"], mesh.shape["tp"]),
        mesh=mesh,
        in_specs=(matrix, matrix, partial, row, column) * 4,
        out_specs=(matrix, matrix, row, column) * 4,
        check_vma=False,
    )
```

```python
import functools

import jax
import jax.numpy as jnp
from jax import lax
from jax.experimental import pallas as pl
from jax.experimental.pallas import tpu as pltpu
from jax.sharding import PartitionSpec as P

momentum_decay = 0.9
moment_decay = 0.95
clip_level = 0.25
step_rate = 0.1
MESH = pl.DeviceIdType.MESH
LANES = 128


class Plan:
    def __init__(self, height, width):
        rows = LANES if height % LANES == 0 else height
        tiles = width // LANES
        if (height // rows) % 2 and tiles % 2:
            rows //= 2
        self.height, self.width, self.rows, self.tiles = height, width, rows, tiles
        self.chunks = height // rows
        self.by_rows = self.chunks % 2 == 0
        self.own_chunks = self.chunks // 2 if self.by_rows else self.chunks
        self.own_tiles = tiles if self.by_rows else tiles // 2
        self.region = (self.own_chunks * rows, self.own_tiles * LANES)
        cut = (self.own_chunks + 1) // 2
        self.pieces = [(0, cut)] + ([(cut, self.own_chunks)] if cut < self.own_chunks else [])

    def row_at(self, owner, c):
        start = (owner * self.own_chunks + c) * self.rows if self.by_rows else c * self.rows
        return pl.multiple_of(start, self.rows)

    def column_at(self, owner, j=0):
        return j * LANES if self.by_rows else pl.multiple_of((owner * self.own_tiles + j) * LANES, LANES)

    def part(self, owner, first, last):
        return pl.ds(self.row_at(owner, first), (last - first) * self.rows), pl.ds(self.column_at(owner), self.region[1])

    def block(self, owner):
        return pl.ds(self.row_at(owner, 0), self.region[0]), pl.ds(self.column_at(owner), self.region[1])

    def tile(self, owner, c, j):
        return pl.ds(self.row_at(owner, c), self.rows), pl.ds(self.column_at(owner, j), LANES)


def fold(x):
    return jnp.sum(x.reshape(x.shape[0] // 8, 8, x.shape[1]), axis=0)


def to_lanes(x):
    rows = x.shape[0]
    if rows < LANES:
        x = jnp.concatenate([x, jnp.zeros((LANES - rows, LANES), x.dtype)], axis=0)
    return jnp.sum(x.T, axis=0, keepdims=True)


def to_rows(x, rows):
    return jnp.broadcast_to(x, (LANES, LANES)).T[:rows]


def gather_kernel(plans, n_fs, n_tp, *refs):
    n_all = n_fs * n_tp
    ins, refs = refs[:20], refs[20:]
    outs, refs = refs[:20], refs[20:]
    own, refs = refs[:4], refs[4:]
    other, refs = refs[:4], refs[4:]
    row_all, refs = refs[:4], refs[4:]
    column_part, refs = refs[:4], refs[4:]
    column_all, refs = refs[:4], refs[4:]
    row_in, refs = refs[:4], refs[4:]
    column_in, refs = refs[:4], refs[4:]
    (share_all, own_sem, other_send, other_recv, momentum_sem, back_send, back_recv, weight_sem, moment_sem,
     row_send, row_recv, column_send, column_recv, share_send, share_recv, ready, everyone) = refs
    fs, tp, rep = lax.axis_index("fs"), lax.axis_index("tp"), lax.axis_index("rep")
    partner = {"rep": 1 - rep}
    barrier = pltpu.get_barrier_semaphore()

    def rows_of(p, c):
        return pl.ds(pl.multiple_of(c * p.rows, p.rows), p.rows)

    def load(k):
        r, w = plans[k].block(rep)
        return pltpu.make_async_copy(ins[5 * k + 2].at[0, r, w], own[k], own_sem.at[k])

    def load_momentum(k):
        at = plans[k].block(rep)
        return pltpu.make_async_copy(ins[5 * k + 1].at[at], outs[5 * k + 1].at[at], momentum_sem.at[k])

    def send(k, i):
        p = plans[k]
        first, last = p.pieces[i]
        r, w = p.part(1 - rep, first, last)
        return pltpu.make_async_remote_copy(
            src_ref=ins[5 * k + 2].at[0, r, w], dst_ref=other[k].at[pl.ds(first * p.rows, (last - first) * p.rows)],
            send_sem=other_send.at[k], recv_sem=other_recv.at[k, i],
            device_id=partner, device_id_type=MESH)

    def give_back(k, owner):
        at = plans[k].block(owner)
        return pltpu.make_async_remote_copy(
            src_ref=outs[5 * k + 1].at[at], dst_ref=outs[5 * k + 1].at[at],
            send_sem=back_send.at[k], recv_sem=back_recv.at[k],
            device_id=partner, device_id_type=MESH)

    def load_weight(k):
        return pltpu.make_async_copy(ins[5 * k], outs[5 * k], weight_sem.at[k])

    def load_moments(k):
        return (pltpu.make_async_copy(ins[5 * k + 3], row_in[k], moment_sem.at[k]),
                pltpu.make_async_copy(ins[5 * k + 4], column_in[k], moment_sem.at[4 + k]))

    def wait_for(slots, n, sem):
        some = slots.at[pl.ds(0, n)]
        pltpu.make_async_copy(some, some, sem).wait()

    def place(d):
        lin = lax.rem(fs * n_tp + tp + d, n_all)
        return {"fs": lax.div(lin, n_tp), "tp": lax.rem(lin, n_tp)}

    @pl.when(rep == 1)
    def _():
        pl.semaphore_signal(barrier, inc=1, device_id={"rep": 0}, device_id_type=MESH)

    @pl.when(rep == 0)
    def _():
        pl.semaphore_wait(barrier, 1)
        pl.semaphore_signal(ready, inc=1, device_id={"rep": 1}, device_id_type=MESH)

    @pl.when(rep == 1)
    def _():
        pl.semaphore_wait(ready, 1)

    for k, p in enumerate(plans):
        for i in range(len(p.pieces)):
            send(k, i).start()

    @pl.when(rep == 1)
    def _():
        @pl.loop(1, n_all)
        def _(d):
            pl.semaphore_signal(barrier, inc=1, device_id=place(d), device_id_type=MESH)

    for k in range(4):
        load(k).start()
        load_momentum(k).start()
    for k in range(4):
        for copy in load_moments(k):
            copy.start()

    def accumulate(k):
        p = plans[k]
        column_part[k][...] = jnp.zeros_like(column_part[k])
        load(k).wait()
        load_momentum(k).wait()

        def step(c):
            part = jnp.zeros((p.rows, LANES), jnp.float32)
            for j in range(p.own_tiles):
                at = (rows_of(p, c), pl.ds(j * LANES, LANES))
                full = p.tile(rep, c, j)
                grad = own[k][at] + other[k][at]
                outs[5 * k + 1][full] = momentum_decay * outs[5 * k + 1][full] + (1.0 - momentum_decay) * grad
                square = grad * grad
                part = part + square
                column_part[k][:, pl.ds(j * LANES, LANES)] += fold(square)
            row_all[k][rep * n_tp + tp, pl.ds(c, 1)] = to_lanes(part)

        for i, (first, last) in enumerate(p.pieces):
            send(k, i).wait_recv()
            pl.loop(first, last)(step)

        for j in range(p.own_tiles):
            column_all[k][rep * n_fs + fs, pl.ds(j, 1)] = jnp.sum(
                column_part[k][:, pl.ds(j * LANES, LANES)], axis=0, keepdims=True)

    def row_copy(k, d):
        lin = lax.rem(rep * n_tp + tp + d, 2 * n_tp)
        return pltpu.make_async_remote_copy(
            src_ref=row_all[k].at[rep * n_tp + tp], dst_ref=row_all[k].at[rep * n_tp + tp],
            send_sem=row_send.at[k], recv_sem=row_recv.at[k],
            device_id={"rep": lax.div(lin, n_tp), "tp": lax.rem(lin, n_tp)}, device_id_type=MESH)

    def column_copy(k, d):
        lin = lax.rem(rep * n_fs + fs + d, 2 * n_fs)
        return pltpu.make_async_remote_copy(
            src_ref=column_all[k].at[rep * n_fs + fs], dst_ref=column_all[k].at[rep * n_fs + fs],
            send_sem=column_send.at[k], recv_sem=column_recv.at[k],
            device_id={"rep": lax.div(lin, n_fs), "fs": lax.rem(lin, n_fs)}, device_id_type=MESH)

    me = (fs * n_tp + tp) * 2 + rep

    def share_copy(d):
        lin = lax.rem(me + d, 2 * n_all)
        at = lax.div(lin, 2)
        return pltpu.make_async_remote_copy(
            src_ref=share_all.at[me], dst_ref=share_all.at[me],
            send_sem=share_send, recv_sem=share_recv,
            device_id={"rep": lax.rem(lin, 2), "fs": lax.div(at, n_tp), "tp": lax.rem(at, n_tp)},
            device_id_type=MESH)

    def moments(k):
        p = plans[k]

        wait_for(row_all[k], 2 * n_tp - 1, row_recv.at[k])
        wait_for(column_all[k], 2 * n_fs - 1, column_recv.at[k])
        for copy in load_moments(k):
            copy.wait()
        row_sums = [jnp.sum(row_all[k][pl.ds(q * n_tp, n_tp)], axis=0) for q in range(2)]
        column_sums = [jnp.sum(column_all[k][pl.ds(q * n_fs, n_fs)], axis=0) for q in range(2)]
        row_scale = (1.0 - moment_decay) / (p.width * n_tp)
        column_scale = (1.0 - moment_decay) / (p.height * n_fs)
        if p.by_rows:
            for q in range(2):
                at = pl.ds(q * p.own_chunks, p.own_chunks)
                outs[5 * k + 2][at] = moment_decay * row_in[k][at] + row_scale * row_sums[q]
            outs[5 * k + 3][...] = moment_decay * column_in[k][...] + column_scale * (column_sums[0] + column_sums[1])
            mine = outs[5 * k + 2][pl.ds(rep * p.own_chunks, p.own_chunks)]
        else:
            outs[5 * k + 2][...] = moment_decay * row_in[k][...] + row_scale * (row_sums[0] + row_sums[1])
            for q in range(2):
                at = pl.ds(q * p.own_tiles, p.own_tiles)
                outs[5 * k + 3][at] = moment_decay * column_in[k][at] + column_scale * column_sums[q]
            mine = outs[5 * k + 2][...]
        lane = lax.broadcasted_iota(jnp.int32, mine.shape, 1)
        mass = jnp.sum(jnp.where(lane < p.rows, mine, 0.0), axis=0, keepdims=True)
        first_chunk = rep * p.own_chunks if p.by_rows else 0
        first_tile = 0 if p.by_rows else rep * p.own_tiles

        def step(c, sums):
            inverse = to_rows(1.0 / outs[5 * k + 2][pl.ds(first_chunk + c, 1)], p.rows)
            new = []
            for j in range(p.own_tiles):
                m = outs[5 * k + 1][p.tile(rep, c, j)]
                new.append(sums[j] + fold(m * m * inverse))
            return tuple(new)

        zero = jnp.zeros((8, LANES), jnp.float32)
        sums = lax.fori_loop(0, p.own_chunks, step, (zero,) * p.own_tiles)
        share = zero
        for j in range(p.own_tiles):
            share = share + sums[j] / outs[5 * k + 3][pl.ds(first_tile + j, 1)]
        share = jnp.sum(jnp.sum(share, axis=0, keepdims=True), axis=1, keepdims=True)
        return share, jnp.sum(mass, axis=1, keepdims=True)

    for k in range(4):
        accumulate(k)
        if k == 0:
            @pl.when(rep == 1)
            def _():
                pl.semaphore_wait(barrier, n_all - 1)
                pl.semaphore_signal(everyone, inc=1, device_id={"rep": 0}, device_id_type=MESH)

            @pl.when(rep == 0)
            def _():
                pl.semaphore_wait(everyone, 1)

        @pl.loop(1, 2 * n_fs)
        def _(d):
            column_copy(k, d).start()

        @pl.loop(1, 2 * n_tp)
        def _(d):
            row_copy(k, d).start()

    for k in range(4):
        give_back(k, rep).start()
    for k in range(4):
        load_weight(k).start()
    lane = lax.broadcasted_iota(jnp.int32, (1, LANES), 1)
    packed = jnp.zeros((1, LANES), jnp.float32)
    for k in range(4):
        share, mass = moments(k)
        packed = jnp.where(lane == 2 * k, share, jnp.where(lane == 2 * k + 1, mass, packed))
    share_all[me] = packed

    @pl.loop(1, 2 * n_all)
    def _(d):
        share_copy(d).start()

    wait_for(share_all, 2 * n_all - 1, share_recv)

    total = jnp.sum(share_all[...], axis=0)
    totals = [jnp.sum(jnp.where(lane == i, total, 0.0), axis=1, keepdims=True) for i in range(8)]
    for k, p in enumerate(plans):
        copies = n_tp if p.by_rows else 2 * n_tp
        row_mean = totals[2 * k + 1] / (p.height * n_fs * copies)
        spread = jnp.sqrt(row_mean * totals[2 * k] / (p.height * n_fs * p.width * n_tp))
        factor = jnp.maximum(1.0, spread / clip_level)
        outs[5 * k + 4][...] = jnp.broadcast_to(step_rate * jnp.sqrt(row_mean) / factor, (1, LANES))

    for k in range(4):
        load_weight(k).wait()
        give_back(k, 1 - rep).wait_recv()
        give_back(k, rep).wait_send()
        pltpu.make_async_copy(other[k], other[k], other_send.at[k]).wait()
        wait_for(row_all[k], 2 * n_tp - 1, row_send.at[k])
        wait_for(column_all[k], 2 * n_fs - 1, column_send.at[k])
    wait_for(share_all, 2 * n_all - 1, share_send)


def write_kernel(plans, *refs):
    ins, refs = refs[:20], refs[20:]
    outs, refs = refs[:16], refs[16:]
    weight_next, refs = refs[:4], refs[4:]
    momentum_sem, weight_sem = refs

    def put_momentum(k):
        return pltpu.make_async_copy(ins[5 * k + 1], outs[4 * k + 1], momentum_sem.at[k])

    def span(p, c):
        return pl.ds(pl.multiple_of(c * p.rows, p.rows), p.rows)

    def put_weight(k, c):
        return pltpu.make_async_copy(
            weight_next[k].at[span(plans[k], c)], outs[4 * k].at[span(plans[k], c)], weight_sem.at[k])

    for k in range(4):
        put_momentum(k).start()
    for k, p in enumerate(plans):
        outs[4 * k + 2][...] = ins[5 * k + 2][:, :p.rows]
        outs[4 * k + 3][...] = ins[5 * k + 3][...]

        @pl.loop(0, p.chunks)
        def _(c):
            row_factor = to_rows(lax.rsqrt(ins[5 * k + 2][pl.ds(c, 1)]), p.rows)
            for j in range(p.tiles):
                at = (span(p, c), pl.ds(j * LANES, LANES))
                column_factor = lax.rsqrt(ins[5 * k + 3][pl.ds(j, 1)]) * ins[5 * k + 4][...]
                weight_next[k][at] = ins[5 * k][at] - ins[5 * k + 1][at] * row_factor * column_factor
            put_weight(k, c).start()

    for k in range(4):
        put_momentum(k).wait()
        pltpu.make_async_copy(weight_next[k], outs[4 * k], weight_sem.at[k]).wait()


def body(n_fs, n_tp, *arrays):
    f32 = jnp.float32
    plans = tuple(Plan(*arrays[5 * k].shape) for k in range(4))
    n_all = n_fs * n_tp
    operands, middle = [], []
    in_specs = []
    hbm, vmem = pl.BlockSpec(memory_space=pl.ANY), pl.BlockSpec(memory_space=pltpu.VMEM)
    for k, p in enumerate(plans):
        w, m, g, r, c = arrays[5 * k:5 * k + 5]
        r = r.reshape(p.chunks, p.rows)
        if p.rows < LANES:
            r = jnp.pad(r, ((0, 0), (0, LANES - p.rows)), constant_values=1.0)
        c = c.reshape(p.tiles, LANES)
        operands += [pltpu.with_memory_space_constraint(x, pltpu.HBM) for x in (w, m, g, r, c)]
        in_specs += [hbm] * 5
        full = (p.height, p.width)
        middle += [pltpu.VMEM(full, f32), pltpu.VMEM(full, f32),
                   pltpu.VMEM((p.chunks, LANES), f32), pltpu.VMEM((p.tiles, LANES), f32), pltpu.VMEM((1, LANES), f32)]
    scratch = [pltpu.VMEM(p.region, f32) for p in plans] * 2
    scratch += [pltpu.VMEM((2 * n_tp, p.own_chunks, LANES), f32) for p in plans]
    scratch += [pltpu.VMEM((8, p.region[1]), f32) for p in plans]
    scratch += [pltpu.VMEM((2 * n_fs, p.own_tiles, LANES), f32) for p in plans]
    scratch += [pltpu.VMEM((p.chunks, LANES), f32) for p in plans]
    scratch += [pltpu.VMEM((p.tiles, LANES), f32) for p in plans]
    scratch += [pltpu.VMEM((2 * n_all, 1, LANES), f32)]
    dma = pltpu.SemaphoreType.DMA
    scratch += [dma((4,))] * 2 + [dma((4, 2))] + [dma((4,))] * 4 + [dma((8,))] + [dma((4,))] * 4 + [dma, dma]
    scratch += [pltpu.SemaphoreType.REGULAR, pltpu.SemaphoreType.REGULAR]
    block = 4 * sum(p.height * p.width for p in plans)
    slack = 8 << 20
    middle = pl.pallas_call(
        functools.partial(gather_kernel, plans, n_fs, n_tp),
        out_shape=middle,
        in_specs=in_specs,
        out_specs=[vmem] * 20,
        scratch_shapes=scratch,
        compiler_params=pltpu.CompilerParams(
            collective_id=0, has_side_effects=True, vmem_limit_bytes=block + slack),
        name="gather",
    )(*operands)
    out_shape, out_specs = [], []
    for p in plans:
        out_shape += [jax.ShapeDtypeStruct((p.height, p.width), f32)] * 2
        out_shape += [jax.ShapeDtypeStruct((p.chunks, p.rows), f32), jax.ShapeDtypeStruct((p.tiles, LANES), f32)]
        out_specs += [hbm, hbm, vmem, vmem]
    outs = pl.pallas_call(
        functools.partial(write_kernel, plans),
        out_shape=out_shape,
        in_specs=[vmem] * 20,
        out_specs=out_specs,
        scratch_shapes=[pltpu.VMEM((p.height, p.width), f32) for p in plans] + [dma((4,)), dma((4,))],
        compiler_params=pltpu.CompilerParams(vmem_limit_bytes=block + slack),
        name="write",
    )(*middle)
    results = []
    for k in range(4):
        results += [outs[4 * k], outs[4 * k + 1], outs[4 * k + 2].reshape(-1), outs[4 * k + 3].reshape(-1)]
    return tuple(results)


def solution(mesh):
    matrix, partial, row, column = P("fs", "tp"), P("rep", "fs", "tp"), P("fs"), P("tp")
    return jax.shard_map(
        functools.partial(body, mesh.shape["fs"], mesh.shape["tp"]),
        mesh=mesh,
        in_specs=(matrix, matrix, partial, row, column) * 4,
        out_specs=(matrix, matrix, row, column) * 4,
        check_vma=False,
    )
```

```python
import functools

import jax
import jax.numpy as jnp
from jax import lax
from jax.experimental import pallas as pl
from jax.experimental.pallas import tpu as pltpu
from jax.sharding import PartitionSpec as P

momentum_decay = 0.9
moment_decay = 0.95
clip_level = 0.25
step_rate = 0.1
MESH = pl.DeviceIdType.MESH
LANES = 128
ORDER = (2, 0, 1, 3)


class Plan:
    def __init__(self, height, width):
        rows = LANES if height % LANES == 0 else height
        tiles = width // LANES
        if (height // rows) % 2 and tiles % 2:
            rows //= 2
        self.height, self.width, self.rows, self.tiles = height, width, rows, tiles
        self.chunks = height // rows
        self.by_rows = self.chunks % 2 == 0
        self.own_chunks = self.chunks // 2 if self.by_rows else self.chunks
        self.own_tiles = tiles if self.by_rows else tiles // 2
        self.region = (self.own_chunks * rows, self.own_tiles * LANES)
        cut = (self.own_chunks + 1) // 2
        self.pieces = [(0, cut)] + ([(cut, self.own_chunks)] if cut < self.own_chunks else [])

    def row_at(self, owner, c):
        start = (owner * self.own_chunks + c) * self.rows if self.by_rows else c * self.rows
        return pl.multiple_of(start, self.rows)

    def column_at(self, owner, j=0):
        return j * LANES if self.by_rows else pl.multiple_of((owner * self.own_tiles + j) * LANES, LANES)

    def part(self, owner, first, last):
        return pl.ds(self.row_at(owner, first), (last - first) * self.rows), pl.ds(self.column_at(owner), self.region[1])

    def block(self, owner):
        return pl.ds(self.row_at(owner, 0), self.region[0]), pl.ds(self.column_at(owner), self.region[1])

    def tile(self, owner, c, j):
        return pl.ds(self.row_at(owner, c), self.rows), pl.ds(self.column_at(owner, j), LANES)


def fold(x):
    return jnp.sum(x.reshape(x.shape[0] // 8, 8, x.shape[1]), axis=0)


def to_lanes(x):
    rows = x.shape[0]
    if rows < LANES:
        x = jnp.concatenate([x, jnp.zeros((LANES - rows, LANES), x.dtype)], axis=0)
    return jnp.sum(x.T, axis=0, keepdims=True)


def to_rows(x, rows):
    return jnp.broadcast_to(x, (LANES, LANES)).T[:rows]


def gather_kernel(plans, n_fs, n_tp, *refs):
    n_all = n_fs * n_tp
    ins, refs = refs[:20], refs[20:]
    outs, refs = refs[:20], refs[20:]
    own, refs = refs[:4], refs[4:]
    other, refs = refs[:4], refs[4:]
    row_all, refs = refs[:4], refs[4:]
    column_part, refs = refs[:4], refs[4:]
    column_all, refs = refs[:4], refs[4:]
    row_in, refs = refs[:4], refs[4:]
    column_in, refs = refs[:4], refs[4:]
    (share_all, own_sem, other_send, other_recv, momentum_sem, back_send, back_recv, weight_sem, moment_sem,
     row_send, row_recv, column_send, column_recv, share_send, share_recv, ready, everyone) = refs
    fs, tp, rep = lax.axis_index("fs"), lax.axis_index("tp"), lax.axis_index("rep")
    partner = {"rep": 1 - rep}
    barrier = pltpu.get_barrier_semaphore()

    def rows_of(p, c):
        return pl.ds(pl.multiple_of(c * p.rows, p.rows), p.rows)

    def load(k):
        r, w = plans[k].block(rep)
        return pltpu.make_async_copy(ins[5 * k + 2].at[0, r, w], own[k], own_sem.at[k])

    def load_momentum(k):
        at = plans[k].block(rep)
        return pltpu.make_async_copy(ins[5 * k + 1].at[at], outs[5 * k + 1].at[at], momentum_sem.at[k])

    def send(k, i):
        p = plans[k]
        first, last = p.pieces[i]
        r, w = p.part(1 - rep, first, last)
        return pltpu.make_async_remote_copy(
            src_ref=ins[5 * k + 2].at[0, r, w], dst_ref=other[k].at[pl.ds(first * p.rows, (last - first) * p.rows)],
            send_sem=other_send.at[k], recv_sem=other_recv.at[k, i],
            device_id=partner, device_id_type=MESH)

    def give_back(k, owner):
        at = plans[k].block(owner)
        return pltpu.make_async_remote_copy(
            src_ref=outs[5 * k + 1].at[at], dst_ref=outs[5 * k + 1].at[at],
            send_sem=back_send.at[k], recv_sem=back_recv.at[k],
            device_id=partner, device_id_type=MESH)

    def load_weight(k):
        return pltpu.make_async_copy(ins[5 * k], outs[5 * k], weight_sem.at[k])

    def load_moments(k):
        return (pltpu.make_async_copy(ins[5 * k + 3], row_in[k], moment_sem.at[k]),
                pltpu.make_async_copy(ins[5 * k + 4], column_in[k], moment_sem.at[4 + k]))

    def wait_for(slots, n, sem):
        some = slots.at[pl.ds(0, n)]
        pltpu.make_async_copy(some, some, sem).wait()

    def place(d):
        lin = lax.rem(fs * n_tp + tp + d, n_all)
        return {"fs": lax.div(lin, n_tp), "tp": lax.rem(lin, n_tp)}

    @pl.when(rep == 1)
    def _():
        pl.semaphore_signal(barrier, inc=1, device_id={"rep": 0}, device_id_type=MESH)

    @pl.when(rep == 0)
    def _():
        pl.semaphore_wait(barrier, 1)
        pl.semaphore_signal(ready, inc=1, device_id={"rep": 1}, device_id_type=MESH)

    @pl.when(rep == 1)
    def _():
        pl.semaphore_wait(ready, 1)

    for k in ORDER:
        for i in range(len(plans[k].pieces)):
            send(k, i).start()

    @pl.when(rep == 1)
    def _():
        @pl.loop(1, n_all)
        def _(d):
            pl.semaphore_signal(barrier, inc=1, device_id=place(d), device_id_type=MESH)

    for k in ORDER:
        load(k).start()
        load_momentum(k).start()
    for k in range(4):
        for copy in load_moments(k):
            copy.start()

    def accumulate(k):
        p = plans[k]
        column_part[k][...] = jnp.zeros_like(column_part[k])
        load(k).wait()
        load_momentum(k).wait()

        def step(c):
            part = jnp.zeros((p.rows, LANES), jnp.float32)
            for j in range(p.own_tiles):
                at = (rows_of(p, c), pl.ds(j * LANES, LANES))
                full = p.tile(rep, c, j)
                grad = own[k][at] + other[k][at]
                outs[5 * k + 1][full] = momentum_decay * outs[5 * k + 1][full] + (1.0 - momentum_decay) * grad
                square = grad * grad
                part = part + square
                column_part[k][:, pl.ds(j * LANES, LANES)] += fold(square)
            row_all[k][rep * n_tp + tp, pl.ds(c, 1)] = to_lanes(part)

        for i, (first, last) in enumerate(p.pieces):
            send(k, i).wait_recv()
            pl.loop(first, last)(step)

        for j in range(p.own_tiles):
            column_all[k][rep * n_fs + fs, pl.ds(j, 1)] = jnp.sum(
                column_part[k][:, pl.ds(j * LANES, LANES)], axis=0, keepdims=True)

    def row_copy(k, d):
        lin = lax.rem(rep * n_tp + tp + d, 2 * n_tp)
        return pltpu.make_async_remote_copy(
            src_ref=row_all[k].at[rep * n_tp + tp], dst_ref=row_all[k].at[rep * n_tp + tp],
            send_sem=row_send.at[k], recv_sem=row_recv.at[k],
            device_id={"rep": lax.div(lin, n_tp), "tp": lax.rem(lin, n_tp)}, device_id_type=MESH)

    def column_copy(k, d):
        lin = lax.rem(rep * n_fs + fs + d, 2 * n_fs)
        return pltpu.make_async_remote_copy(
            src_ref=column_all[k].at[rep * n_fs + fs], dst_ref=column_all[k].at[rep * n_fs + fs],
            send_sem=column_send.at[k], recv_sem=column_recv.at[k],
            device_id={"rep": lax.div(lin, n_fs), "fs": lax.rem(lin, n_fs)}, device_id_type=MESH)

    me = (fs * n_tp + tp) * 2 + rep

    def share_copy(d):
        lin = lax.rem(me + d, 2 * n_all)
        at = lax.div(lin, 2)
        return pltpu.make_async_remote_copy(
            src_ref=share_all.at[me], dst_ref=share_all.at[me],
            send_sem=share_send, recv_sem=share_recv,
            device_id={"rep": lax.rem(lin, 2), "fs": lax.div(at, n_tp), "tp": lax.rem(at, n_tp)},
            device_id_type=MESH)

    def moments(k):
        p = plans[k]

        wait_for(row_all[k], 2 * n_tp - 1, row_recv.at[k])
        wait_for(column_all[k], 2 * n_fs - 1, column_recv.at[k])
        for copy in load_moments(k):
            copy.wait()
        row_sums = [jnp.sum(row_all[k][pl.ds(q * n_tp, n_tp)], axis=0) for q in range(2)]
        column_sums = [jnp.sum(column_all[k][pl.ds(q * n_fs, n_fs)], axis=0) for q in range(2)]
        row_scale = (1.0 - moment_decay) / (p.width * n_tp)
        column_scale = (1.0 - moment_decay) / (p.height * n_fs)
        if p.by_rows:
            for q in range(2):
                at = pl.ds(q * p.own_chunks, p.own_chunks)
                outs[5 * k + 2][at] = moment_decay * row_in[k][at] + row_scale * row_sums[q]
            outs[5 * k + 3][...] = moment_decay * column_in[k][...] + column_scale * (column_sums[0] + column_sums[1])
            mine = outs[5 * k + 2][pl.ds(rep * p.own_chunks, p.own_chunks)]
        else:
            outs[5 * k + 2][...] = moment_decay * row_in[k][...] + row_scale * (row_sums[0] + row_sums[1])
            for q in range(2):
                at = pl.ds(q * p.own_tiles, p.own_tiles)
                outs[5 * k + 3][at] = moment_decay * column_in[k][at] + column_scale * column_sums[q]
            mine = outs[5 * k + 2][...]
        lane = lax.broadcasted_iota(jnp.int32, mine.shape, 1)
        mass = jnp.sum(jnp.where(lane < p.rows, mine, 0.0), axis=0, keepdims=True)
        first_chunk = rep * p.own_chunks if p.by_rows else 0
        first_tile = 0 if p.by_rows else rep * p.own_tiles

        def step(c, sums):
            inverse = to_rows(1.0 / outs[5 * k + 2][pl.ds(first_chunk + c, 1)], p.rows)
            new = []
            for j in range(p.own_tiles):
                m = outs[5 * k + 1][p.tile(rep, c, j)]
                new.append(sums[j] + fold(m * m * inverse))
            return tuple(new)

        zero = jnp.zeros((8, LANES), jnp.float32)
        sums = lax.fori_loop(0, p.own_chunks, step, (zero,) * p.own_tiles)
        share = zero
        for j in range(p.own_tiles):
            share = share + sums[j] / outs[5 * k + 3][pl.ds(first_tile + j, 1)]
        share = jnp.sum(jnp.sum(share, axis=0, keepdims=True), axis=1, keepdims=True)
        return share, jnp.sum(mass, axis=1, keepdims=True)

    for k in ORDER:
        accumulate(k)
        if k == ORDER[0]:
            @pl.when(rep == 1)
            def _():
                pl.semaphore_wait(barrier, n_all - 1)
                pl.semaphore_signal(everyone, inc=1, device_id={"rep": 0}, device_id_type=MESH)

            @pl.when(rep == 0)
            def _():
                pl.semaphore_wait(everyone, 1)

        @pl.loop(1, 2 * n_fs)
        def _(d):
            column_copy(k, d).start()

        @pl.loop(1, 2 * n_tp)
        def _(d):
            row_copy(k, d).start()

    for k in range(4):
        give_back(k, rep).start()
    for k in range(4):
        load_weight(k).start()
    lane = lax.broadcasted_iota(jnp.int32, (1, LANES), 1)
    packed = jnp.zeros((1, LANES), jnp.float32)
    for k in ORDER:
        share, mass = moments(k)
        packed = jnp.where(lane == 2 * k, share, jnp.where(lane == 2 * k + 1, mass, packed))
    share_all[me] = packed

    @pl.loop(1, 2 * n_all)
    def _(d):
        share_copy(d).start()

    wait_for(share_all, 2 * n_all - 1, share_recv)

    total = jnp.sum(share_all[...], axis=0)
    totals = [jnp.sum(jnp.where(lane == i, total, 0.0), axis=1, keepdims=True) for i in range(8)]
    for k, p in enumerate(plans):
        copies = n_tp if p.by_rows else 2 * n_tp
        row_mean = totals[2 * k + 1] / (p.height * n_fs * copies)
        spread = jnp.sqrt(row_mean * totals[2 * k] / (p.height * n_fs * p.width * n_tp))
        factor = jnp.maximum(1.0, spread / clip_level)
        outs[5 * k + 4][...] = jnp.broadcast_to(step_rate * jnp.sqrt(row_mean) / factor, (1, LANES))

    for k in range(4):
        load_weight(k).wait()
        give_back(k, 1 - rep).wait_recv()
        give_back(k, rep).wait_send()
        pltpu.make_async_copy(other[k], other[k], other_send.at[k]).wait()
        wait_for(row_all[k], 2 * n_tp - 1, row_send.at[k])
        wait_for(column_all[k], 2 * n_fs - 1, column_send.at[k])
    wait_for(share_all, 2 * n_all - 1, share_send)


def write_kernel(plans, *refs):
    ins, refs = refs[:20], refs[20:]
    outs, refs = refs[:16], refs[16:]
    weight_next, refs = refs[:4], refs[4:]
    momentum_sem, weight_sem = refs

    def put_momentum(k):
        return pltpu.make_async_copy(ins[5 * k + 1], outs[4 * k + 1], momentum_sem.at[k])

    def span(p, c):
        return pl.ds(pl.multiple_of(c * p.rows, p.rows), p.rows)

    def put_weight(k, c):
        return pltpu.make_async_copy(
            weight_next[k].at[span(plans[k], c)], outs[4 * k].at[span(plans[k], c)], weight_sem.at[k])

    for k in range(4):
        put_momentum(k).start()
    for k, p in enumerate(plans):
        outs[4 * k + 2][...] = ins[5 * k + 2][:, :p.rows]
        outs[4 * k + 3][...] = ins[5 * k + 3][...]

        @pl.loop(0, p.chunks)
        def _(c):
            row_factor = to_rows(lax.rsqrt(ins[5 * k + 2][pl.ds(c, 1)]), p.rows)
            for j in range(p.tiles):
                at = (span(p, c), pl.ds(j * LANES, LANES))
                column_factor = lax.rsqrt(ins[5 * k + 3][pl.ds(j, 1)]) * ins[5 * k + 4][...]
                weight_next[k][at] = ins[5 * k][at] - ins[5 * k + 1][at] * row_factor * column_factor
            put_weight(k, c).start()

    for k in range(4):
        put_momentum(k).wait()
        pltpu.make_async_copy(weight_next[k], outs[4 * k], weight_sem.at[k]).wait()


def body(n_fs, n_tp, *arrays):
    f32 = jnp.float32
    plans = tuple(Plan(*arrays[5 * k].shape) for k in range(4))
    n_all = n_fs * n_tp
    operands, middle = [], []
    in_specs = []
    hbm, vmem = pl.BlockSpec(memory_space=pl.ANY), pl.BlockSpec(memory_space=pltpu.VMEM)
    for k, p in enumerate(plans):
        w, m, g, r, c = arrays[5 * k:5 * k + 5]
        r = r.reshape(p.chunks, p.rows)
        if p.rows < LANES:
            r = jnp.pad(r, ((0, 0), (0, LANES - p.rows)), constant_values=1.0)
        c = c.reshape(p.tiles, LANES)
        operands += [pltpu.with_memory_space_constraint(x, pltpu.HBM) for x in (w, m, g, r, c)]
        in_specs += [hbm] * 5
        full = (p.height, p.width)
        middle += [pltpu.VMEM(full, f32), pltpu.VMEM(full, f32),
                   pltpu.VMEM((p.chunks, LANES), f32), pltpu.VMEM((p.tiles, LANES), f32), pltpu.VMEM((1, LANES), f32)]
    scratch = [pltpu.VMEM(p.region, f32) for p in plans] * 2
    scratch += [pltpu.VMEM((2 * n_tp, p.own_chunks, LANES), f32) for p in plans]
    scratch += [pltpu.VMEM((8, p.region[1]), f32) for p in plans]
    scratch += [pltpu.VMEM((2 * n_fs, p.own_tiles, LANES), f32) for p in plans]
    scratch += [pltpu.VMEM((p.chunks, LANES), f32) for p in plans]
    scratch += [pltpu.VMEM((p.tiles, LANES), f32) for p in plans]
    scratch += [pltpu.VMEM((2 * n_all, 1, LANES), f32)]
    dma = pltpu.SemaphoreType.DMA
    scratch += [dma((4,))] * 2 + [dma((4, 2))] + [dma((4,))] * 4 + [dma((8,))] + [dma((4,))] * 4 + [dma, dma]
    scratch += [pltpu.SemaphoreType.REGULAR, pltpu.SemaphoreType.REGULAR]
    block = 4 * sum(p.height * p.width for p in plans)
    slack = 8 << 20
    middle = pl.pallas_call(
        functools.partial(gather_kernel, plans, n_fs, n_tp),
        out_shape=middle,
        in_specs=in_specs,
        out_specs=[vmem] * 20,
        scratch_shapes=scratch,
        compiler_params=pltpu.CompilerParams(
            collective_id=0, has_side_effects=True, vmem_limit_bytes=block + slack),
        name="gather",
    )(*operands)
    out_shape, out_specs = [], []
    for p in plans:
        out_shape += [jax.ShapeDtypeStruct((p.height, p.width), f32)] * 2
        out_shape += [jax.ShapeDtypeStruct((p.chunks, p.rows), f32), jax.ShapeDtypeStruct((p.tiles, LANES), f32)]
        out_specs += [hbm, hbm, vmem, vmem]
    outs = pl.pallas_call(
        functools.partial(write_kernel, plans),
        out_shape=out_shape,
        in_specs=[vmem] * 20,
        out_specs=out_specs,
        scratch_shapes=[pltpu.VMEM((p.height, p.width), f32) for p in plans] + [dma((4,)), dma((4,))],
        compiler_params=pltpu.CompilerParams(vmem_limit_bytes=block + slack),
        name="write",
    )(*middle)
    results = []
    for k in range(4):
        results += [outs[4 * k], outs[4 * k + 1], outs[4 * k + 2].reshape(-1), outs[4 * k + 3].reshape(-1)]
    return tuple(results)


def solution(mesh):
    matrix, partial, row, column = P("fs", "tp"), P("rep", "fs", "tp"), P("fs"), P("tp")
    return jax.shard_map(
        functools.partial(body, mesh.shape["fs"], mesh.shape["tp"]),
        mesh=mesh,
        in_specs=(matrix, matrix, partial, row, column) * 4,
        out_specs=(matrix, matrix, row, column) * 4,
        check_vma=False,
    )
```
